128 devices in a mesh: sp: 32 (over z, y, core), tp: 4 (over x).
Axes of the slice: x: 4, y: 4, z: 4, core: 2. Of those that a mesh axis runs over, the one named last changes fastest.
Arguments:
- tokens: bfloat16 [32768, 2048], P(('sp', 'tp')), may hold values from -6 to 6
- norm_gain: float32 [2048], replicated, may hold values from 0.1 to 1.9
- w_query: bfloat16 [2048, 2048], P(None, 'tp'), may hold values from -0.125 to 0.125
- w_forget: bfloat16 [2048, 2048], P(None, 'tp'), may hold values from -0.125 to 0.125
- w_value: bfloat16 [2048, 2048], P(None, 'tp'), may hold values from -0.125 to 0.125
- w_rgate: bfloat16 [2048, 2048], P(None, 'tp'), may hold values from -0.125 to 0.125
- w_glu_value: bfloat16 [2048, 2048], P(None, 'tp'), may hold values from -0.125 to 0.125
- w_glu_gate: bfloat16 [2048, 2048], P(None, 'tp'), may hold values from -0.125 to 0.125
- forget_gap: float32 [2048], P('tp'), may hold values from 1.5258789e-05 to 0.1
- decay_shift: float32 [32768, 16], P('sp', 'tp'), may hold values from -0.6 to 0, as said below
- head_gain: float32 [128], replicated, may hold values from 0.1 to 1.9
- conv_taps: float32 [31, 2048], P(None, 'tp'), may hold values from -12 to 12
- conv_gain: float32 [2048], P('tp'), may hold values from 0.1 to 1.9
- out_rec: bfloat16 [2048, 2048], P('tp'), may hold values from -0.09375 to 0.09375
- out_conv: bfloat16 [2048, 2048], P('tp'), may hold values from -0.09375 to 0.09375
Outputs:
- mixed: bfloat16 [32768, 2048], P(('sp', 'tp'))
The draws below stay inside these ranges and needn't reach their ends.
Inputs may be any that keep to these rules, and one draw needn't show every extreme that they name: `decay_shift`: at most zero everywhere.
All inputs are finite; a program needn't handle non-finite values.
Results may differ from the reference program's by a relative error of at most 0.015.
Values may be sent and summed in bfloat16 or wider, within the bound.
A program may use at most 128 MiB of HBM per device.

```python
import jax
import jax.numpy as jnp
from jax import lax

D = 2048
HEADS = 16
HEAD = 128
DC = 2048
CW = 31
BLOCK = 64
TOK_DEV = 1024
DH = 2048
TOKENS = 32768
N_TP = 4


def draw_forget_gap(key, part):
    order = jax.random.permutation(jax.random.fold_in(key, 3), HEADS)
    fast_count = HEADS // 2
    fast = order < fast_count
    spread = jax.random.uniform(jax.random.fold_in(key, 5), (HEADS, HEAD), jnp.float32)
    slow_gap = jnp.exp(jnp.log(0.5) + spread * jnp.log(3.0)) / TOKENS
    fast_gap = jnp.exp(jnp.log(0.03) + spread * jnp.log(10.0 / 3.0))
    return jnp.where(fast[:, None], fast_gap, slow_gap).reshape(HEADS * HEAD)


def draw_decay_shift(key, part):
    block_total = TOKENS // TOK_DEV
    spread = jax.random.uniform(jax.random.fold_in(key, 7), (block_total, 1), jnp.float32)
    rate = jnp.exp(jnp.log(0.2) + spread * jnp.log(5.0)) / TOKENS
    smooth_part = -jnp.repeat(rate, TOK_DEV, axis=0) * jnp.ones((1, HEADS), jnp.float32)
    positions = jax.random.randint(jax.random.fold_in(key, 11), (2,), 0, TOKENS)
    depth = jax.random.uniform(jax.random.fold_in(key, 13), (2, HEADS), jnp.float32, 0.2, 0.4)
    hits = (jnp.arange(TOKENS)[:, None] == positions[None, :]).astype(jnp.float32)
    return smooth_part + jnp.dot(hits, jnp.log(1.0 - depth))


def draw_conv_taps(key, part):
    channel_rise = jnp.exp(jnp.log(3.0) * jnp.arange(DC).astype(jnp.float32) / DC)
    base = jnp.clip(jax.random.normal(jax.random.fold_in(key, 17), (CW, DC), jnp.float32), -4.0, 4.0)
    spread = jnp.exp(jax.random.uniform(jax.random.fold_in(key, 19), (DC,), jnp.float32, 0.0, jnp.log(10.0)))
    scale = 0.1
    return base * channel_rise * spread * scale


def levels(rng, shape, split, least, top_value):
    factor_of = 1.0
    for dim, blocks in split:
        steps = jax.random.uniform(jax.random.fold_in(jax.random.fold_in(rng, 6), dim), (blocks,), jnp.float32, least / len(split), top_value / len(split))
        factor_of = factor_of * jnp.repeat(jnp.exp(steps), shape[dim] // blocks).reshape((-1,) + (1,) * (len(shape) - 1 - dim))
    return factor_of


def gaussian(rng, dims, scale, most, split=(), kind=jnp.bfloat16):
    level = levels(rng, dims, split, -0.22, 0.18) if split else 1.0
    values = jax.random.normal(rng, dims, jnp.float32) * scale * level
    return jnp.minimum(jnp.maximum(values, -most), most).astype(kind)


def setup_inputs(seed: int = 0) -> dict:
    streams_of = jax.random.split(jax.random.key(seed), 16)
    tokens = gaussian(streams_of[0], (TOKENS, D), 1.0, 6.0, ((0, 128),))
    norm_gain = jnp.clip(1.0 + 0.18 * jax.random.normal(streams_of[1], (D,), jnp.float32), 0.1, 1.9)
    w_query = gaussian(streams_of[2], (D, DH), D ** -0.5, 0.125, ((1, 4),))
    w_forget = gaussian(streams_of[3], (D, DH), D ** -0.5, 0.125, ((1, 4),))
    w_value = gaussian(streams_of[4], (D, DH), D ** -0.5, 0.125, ((1, 4),))
    w_rgate = gaussian(streams_of[5], (D, DH), D ** -0.5, 0.125, ((1, 4),))
    w_glu_value = gaussian(streams_of[6], (D, DC), D ** -0.5, 0.125, ((1, 4),))
    w_glu_gate = gaussian(streams_of[7], (D, DC), D ** -0.5, 0.125, ((1, 4),))
    forget_gap = draw_forget_gap(jax.random.fold_in(streams_of[15], 71), 0)
    decay_shift = draw_decay_shift(jax.random.fold_in(streams_of[15], 71), 0)
    head_gain = jnp.clip(1.0 + 0.18 * jax.random.normal(streams_of[10], (HEAD,), jnp.float32), 0.1, 1.9)
    conv_taps = draw_conv_taps(jax.random.fold_in(streams_of[15], 71), 0)
    conv_gain = jnp.clip(1.0 + 0.18 * jax.random.normal(streams_of[12], (DC,), jnp.float32), 0.1, 1.9)
    out_rec = gaussian(streams_of[13], (DH, D), (DH + DC) ** -0.5, 0.09375, ((0, 4),))
    out_conv = gaussian(streams_of[14], (DC, D), (DH + DC) ** -0.5, 0.09375, ((0, 4),))
    return {"tokens": tokens, "norm_gain": norm_gain, "w_query": w_query, "w_forget": w_forget, "w_value": w_value, "w_rgate": w_rgate, "w_glu_value": w_glu_value, "w_glu_gate": w_glu_gate, "forget_gap": forget_gap, "decay_shift": decay_shift, "head_gain": head_gain, "conv_taps": conv_taps, "conv_gain": conv_gain, "out_rec": out_rec, "out_conv": out_conv}


precise_setting = lax.Precision.HIGHEST
norm_epsilon = 1e-05
head_epsilon = 1e-06

def layer_norm(values, gain):
    widened = values.astype(jnp.float32)
    row_mean = lax.optimization_barrier(jnp.mean(widened, axis=-1, keepdims=True))
    centred = widened - row_mean
    row_var = lax.optimization_barrier(jnp.mean(centred * centred, axis=-1, keepdims=True))
    return centred * lax.rsqrt(row_var + norm_epsilon) * gain.astype(jnp.float32)

def block_scan(query, key_gate, values, log_forget):
    row_count, head_count, key_width = query.shape
    value_width = values.shape[2]
    block_count = row_count // BLOCK

    def to_blocks(array):
        return array.reshape(block_count, BLOCK, head_count, array.shape[2]).transpose(0, 2, 1, 3)
    causal = lax.broadcasted_iota(jnp.int32, (BLOCK, BLOCK), 0) >= lax.broadcasted_iota(jnp.int32, (BLOCK, BLOCK), 1)

    def advance(current_state, inputs):
        query_blk, key_block, value_block, log_blk = inputs
        running_total = jnp.cumsum(log_blk, axis=1)
        closing_log = running_total[:, -1:, :]
        query_decayed = query_blk * jnp.exp(running_total)
        scores = jnp.einsum('htk,hsk->hts', query_decayed, key_block * jnp.exp(-running_total), precision=precise_setting)
        scores = jnp.where(causal[None], scores, 0.0)
        output_rows = jnp.einsum('hts,hsv->htv', scores, value_block, precision=precise_setting)
        output_rows = output_rows + jnp.einsum('ori,oiq->orq', query_decayed, current_state, precision=precise_setting)
        current_state = jnp.exp(closing_log[:, 0, :])[:, :, None] * current_state + jnp.einsum('itp,ito->ipo', key_block * jnp.exp(closing_log - running_total), value_block, precision=precise_setting)
        return (current_state, output_rows)
    start_state = jnp.zeros((head_count, key_width, value_width), jnp.float32)
    final_state, output_rows = lax.scan(advance, start_state, (to_blocks(query), to_blocks(key_gate), to_blocks(values), to_blocks(log_forget)))
    return output_rows.transpose(0, 2, 1, 3).reshape(row_count, head_count, value_width)

def reference(tokens, norm_gain, w_query, w_forget, w_value, w_rgate, w_glu_value, w_glu_gate, forget_gap, decay_shift, head_gain, conv_taps, conv_gain, out_rec, out_conv):
    normed = layer_norm(tokens, norm_gain).astype(jnp.bfloat16)

    def project(weight):
        return jnp.dot(normed, weight, preferred_element_type=jnp.float32).astype(jnp.bfloat16)
    query_raw = project(w_query)
    forget_raw = project(w_forget)
    value_raw = project(w_value)
    rgate_raw = project(w_rgate)
    glu_value = project(w_glu_value)
    glu_gate = project(w_glu_gate)
    seq_len = tokens.shape[0]
    query = jax.nn.silu(query_raw.astype(jnp.float32)).reshape(seq_len, HEADS, HEAD)
    key_gate = forget_gap * jax.nn.sigmoid(-forget_raw.astype(jnp.float32))
    log_forget = jnp.log1p(-key_gate).reshape(seq_len, HEADS, HEAD) + decay_shift[:, :, None]
    values = value_raw.astype(jnp.float32).reshape(seq_len, HEADS, HEAD)
    recurrent_branch = block_scan(query, key_gate.reshape(seq_len, HEADS, HEAD), values, log_forget)
    recurrent_branch = recurrent_branch * lax.rsqrt(lax.optimization_barrier(jnp.mean(recurrent_branch * recurrent_branch, axis=-1, keepdims=True)) + head_epsilon) * head_gain
    rec_out = (recurrent_branch.reshape(seq_len, HEADS * HEAD) * jax.nn.silu(rgate_raw.astype(jnp.float32))).astype(jnp.bfloat16)
    mixed_in = (glu_value.astype(jnp.float32) * jax.nn.sigmoid(glu_gate.astype(jnp.float32))).astype(jnp.bfloat16)
    padded = lax.optimization_barrier(jnp.concatenate([jnp.zeros((CW - 1, DC), jnp.bfloat16), mixed_in], axis=0)).astype(jnp.float32)
    filtered = jnp.zeros((seq_len, DC), jnp.float32)
    for tap_index in range(CW):
        filtered = filtered + conv_taps[tap_index] * padded[tap_index:tap_index + seq_len]
    conv_out = jax.nn.silu(layer_norm(filtered, conv_gain)).astype(jnp.bfloat16)
    rec_share = HEADS * HEAD // N_TP
    conv_share = DC // N_TP
    mixed = jnp.zeros((seq_len, D), jnp.float32)
    for group in range(N_TP):
        term = jnp.dot(rec_out[:, group * rec_share:(group + 1) * rec_share], out_rec[group * rec_share:(group + 1) * rec_share], preferred_element_type=jnp.float32)
        term = term + jnp.dot(conv_out[:, group * conv_share:(group + 1) * conv_share], out_conv[group * conv_share:(group + 1) * conv_share], preferred_element_type=jnp.float32)
        mixed = mixed + lax.optimization_barrier(term.astype(jnp.bfloat16)).astype(jnp.float32)
    return mixed.astype(jnp.bfloat16)
```

```python
import jax
import jax.numpy as jnp
from jax import lax
from jax.experimental import pallas as pl
from jax.experimental.pallas import tpu as pltpu
from jax.sharding import PartitionSpec as P

MESH = pl.DeviceIdType.MESH
HEAD = 128
UNIT = 128
f32 = jnp.float32
bf16 = jnp.bfloat16

norm_epsilon = 1e-05
head_epsilon = 1e-06

NT = (((1,), (1,)), ((), ()))
TN = (((0,), (0,)), ((), ()))


def dot(a, b):
    return jnp.dot(a, b, preferred_element_type=f32)


def split3(value):
    hi = value.astype(bf16)
    rest = value - hi.astype(f32)
    mid = rest.astype(bf16)
    low = (rest - mid.astype(f32)).astype(bf16)
    return hi, mid, low


def pack_state(state, log):
    hi, mid, low = split3(log)
    row = lax.broadcasted_iota(jnp.int32, (16, state.shape[1]), 0)
    extra = jnp.where(
        row == 0,
        hi.astype(f32),
        jnp.where(row == 1, mid.astype(f32), jnp.where(row == 2, low.astype(f32), 0.0)),
    )
    return state.astype(bf16), extra.astype(bf16)


def unpack_state(ref):
    state = ref[0:128, :].astype(f32)
    log = jnp.sum(ref[128:144, :].astype(f32), axis=0, keepdims=True)
    return state, log


def kernel(
    tokens,
    norm_gain,
    w_query,
    w_forget,
    w_value,
    w_rgate,
    w_glu_value,
    w_glu_gate,
    gap,
    shift,
    head_gain,
    taps,
    conv_gain,
    out_rec,
    out_conv,
    out,
    tok,
    xn,
    xp,
    w_in,
    w_out,
    raw,
    hml,
    run,
    keys,
    kdec,
    near,
    qfar,
    rgate,
    pad,
    filt,
    s_unit,
    a_unit,
    h_unit,
    s_loc,
    a_loc,
    p_send,
    p_recv,
    y_msg,
    z_msg,
    h_in,
    stat,
    o_in,
    part,
    s_buf,
    r_buf,
    load_sem,
    ag_send,
    ag_recv,
    sp_send,
    sp_recv,
    st_send,
    st_recv,
    rs_send,
    rs_recv,
):
    x = lax.axis_index("tp")
    s = lax.axis_index("sp")
    core = lax.rem(s, 2)
    chip = s // 2
    y = lax.rem(chip, 4)
    z = chip // 4
    right = lax.rem(x + 1, 4)
    left = lax.rem(x + 3, 4)
    far = lax.rem(x + 2, 4)
    behind = lax.rem(s + 31, 32)
    ahead = lax.rem(s + 1, 32)
    partner = chip * 2 + (1 - core)

    def at_y(k):
        return (z * 4 + lax.rem(y + k, 4)) * 2 + core

    def at_z(k):
        return (lax.rem(z + k, 4) * 4 + y) * 2 + core

    barrier = pltpu.get_barrier_semaphore()
    peers = [{"tp": right}, {"tp": left}, {"tp": far}, {"sp": partner}, {"sp": behind}]
    peers += [{"sp": at_y(k)} for k in (1, 2, 3)] + [{"sp": at_z(k)} for k in (1, 2, 3)]
    for peer in peers:
        pl.semaphore_signal(barrier, inc=1, device_id=peer, device_id_type=MESH)

    loads = [
        pltpu.make_async_copy(tokens, tok, load_sem.at[0]),
    ]
    for k, weight in enumerate((w_forget, w_value, w_query, w_rgate, w_glu_value, w_glu_gate)):
        loads.append(pltpu.make_async_copy(weight, w_in.at[k], load_sem.at[1 + k]))
    loads.append(pltpu.make_async_copy(out_rec, w_out.at[pl.ds(0, 512)], load_sem.at[7]))
    loads.append(pltpu.make_async_copy(out_conv, w_out.at[pl.ds(512, 512)], load_sem.at[8]))
    for load in loads:
        load.start()

    def norm_rows(piece):
        @pl.loop(0, UNIT // 16)
        def _(i):
            row = pl.multiple_of(i * 16, 16)
            wide = tok[pl.ds(piece * UNIT + row, 16), :].astype(f32)
            mean = jnp.mean(wide, axis=1, keepdims=True)
            centred = wide - mean
            var = jnp.mean(centred * centred, axis=1, keepdims=True)
            value = centred * lax.rsqrt(var + norm_epsilon) * norm_gain[...]
            xn[2 * x + piece, pl.ds(row, 16), :] = value.astype(bf16)

    def send_unit(unit, k, target):
        return pltpu.make_async_remote_copy(
            src_ref=xn.at[unit],
            dst_ref=xn.at[unit],
            send_sem=ag_send.at[k],
            recv_sem=ag_recv.at[k],
            device_id={"tp": target},
            device_id_type=MESH,
        )

    gather = [
        send_unit(2 * x, 0, right),
        send_unit(2 * x + 1, 1, right),
        send_unit(2 * left, 2, right),
        send_unit(2 * x + 1, 3, left),
        send_unit(2 * x, 4, left),
        send_unit(2 * right + 1, 5, left),
    ]
    arrive = [
        send_unit(2 * left, 0, right),
        send_unit(2 * left + 1, 1, right),
        send_unit(2 * far, 2, right),
        send_unit(2 * right + 1, 3, left),
        send_unit(2 * right, 4, left),
        send_unit(2 * far + 1, 5, left),
    ]
    loads[0].wait()
    norm_rows(0)
    pl.semaphore_wait(barrier, len(peers))
    gather[0].start()
    norm_rows(1)
    gather[3].start()
    gather[1].start()
    gather[4].start()

    keep = lax.broadcasted_iota(jnp.int32, (UNIT, UNIT), 0) >= lax.broadcasted_iota(
        jnp.int32, (UNIT, UNIT), 1
    )
    ones_low = jnp.where(keep, 1.0, 0.0).astype(bf16)
    tri = jnp.concatenate([ones_low, ones_low, ones_low], axis=1)

    def lanes(h):
        return slice(h * HEAD, (h + 1) * HEAD)

    def sp_copy(src, dst, k, target):
        return pltpu.make_async_remote_copy(
            src_ref=src,
            dst_ref=dst,
            send_sem=sp_send.at[k],
            recv_sem=sp_recv.at[k],
            device_id={"sp": target},
            device_id_type=MESH,
        )

    def pair_copy():
        return sp_copy(p_send, p_recv, 0, partner)

    @pl.loop(0, 4)
    def _(step):
        unit_a = jnp.where(
            step == 0,
            2 * x,
            jnp.where(step == 1, 2 * left, jnp.where(step == 2, 2 * left + 1, 2 * far)),
        )
        unit_b = jnp.where(
            step == 0,
            2 * x + 1,
            jnp.where(step == 1, 2 * right + 1, jnp.where(step == 2, 2 * right, 2 * far + 1)),
        )

        @pl.when(step == 0)
        def _():
            for k in range(1, 7):
                loads[k].wait()

        @pl.when(step == 1)
        def _():
            arrive[0].wait_recv()
            gather[2].start()
            arrive[3].wait_recv()
            gather[5].start()

        @pl.when(step == 2)
        def _():
            arrive[1].wait_recv()
            arrive[4].wait_recv()

        @pl.when(step == 3)
        def _():
            arrive[2].wait_recv()
            arrive[5].wait_recv()

        xp[0:UNIT, :] = xn[unit_a]
        xp[UNIT : 2 * UNIT, :] = xn[unit_b]
        for k in (0, 1):
            raw[k] = dot(xp[...], w_in[k]).astype(bf16)

        @pl.loop(0, 2)
        def _(k):
            unit = jnp.where(k == 0, unit_a, unit_b)
            row = pl.multiple_of(k * UNIT, UNIT)
            rows = pl.ds(row, UNIT)
            for h in range(4):
                forget = raw[0, rows, lanes(h)].astype(f32)
                gate = gap[:, lanes(h)] * jax.nn.sigmoid(-forget)
                in_unit = pl.ds(pl.multiple_of(unit * UNIT, UNIT), UNIT)
                log = jnp.log1p(-gate) + shift[in_unit, h : h + 1]
                hi, mid, low = split3(log)
                hml[0:UNIT, lanes(h)] = hi
                hml[UNIT : 2 * UNIT, lanes(h)] = mid
                hml[2 * UNIT : 3 * UNIT, lanes(h)] = low
                keys[:, lanes(h)] = gate
            total = dot(tri, hml[...])
            run[k] = total
            a_unit[unit] = jnp.broadcast_to(total[UNIT - 1 : UNIT, :], (8, 512))
            for h in range(4):
                run_h = run[k, :, lanes(h)]
                centre = run_h[63:64, :]
                end = run_h[127:128, :]
                decayed = keys[:, lanes(h)] * jnp.exp(centre - run_h)
                kdec[k, :, lanes(h)] = decayed.astype(bf16)
                ending = (decayed * jnp.exp(end - centre)).astype(bf16)
                s_unit[unit, :, lanes(h)] = lax.dot_general(
                    raw[1, rows, lanes(h)], ending, TN, preferred_element_type=f32
                )

        @pl.when(step == 3)
        def _():
            state = s_unit[0]
            log = a_unit[0, 0:1, :]
            for u in range(1, 8):
                a_u = a_unit[u, 0:1, :]
                state = state * jnp.exp(a_u) + s_unit[u]
                log = log + a_u
            for half in range(2):
                part_of = slice(half * 256, half * 256 + 256)
                s_loc[half] = state[:, part_of]
                a_loc[half] = jnp.broadcast_to(log[:, part_of], (8, 256))
            body, extra = pack_state(s_loc[1 - core], a_loc[1 - core, 0:1, :])
            p_send[0:128, :] = body
            p_send[128:144, :] = extra
            pair_copy().start()

        for k in (2, 3, 4, 5):
            raw[k] = dot(xp[...], w_in[k]).astype(bf16)

        @pl.loop(0, 2)
        def _(k):
            unit = jnp.where(k == 0, unit_a, unit_b)
            row = pl.multiple_of(k * UNIT, UNIT)
            rows = pl.ds(row, UNIT)
            for h in range(4):
                run_h = run[k, :, lanes(h)]
                centre = run_h[63:64, :]
                query = raw[2, rows, lanes(h)].astype(f32)
                query = query * jax.nn.sigmoid(query) * jnp.exp(run_h - centre)
                qfar[unit, :, lanes(h)] = (query * jnp.exp(centre)).astype(bf16)
                scores = lax.dot_general(
                    query.astype(bf16), kdec[k, :, lanes(h)], NT, preferred_element_type=f32
                )
                scores = jnp.where(keep, scores, 0.0).astype(bf16)
                near[unit, :, lanes(h)] = dot(scores, raw[1, rows, lanes(h)])
                rgate[unit, :, lanes(h)] = raw[3, rows, lanes(h)]
                value = raw[4, rows, lanes(h)].astype(f32)
                mixed = value * jax.nn.sigmoid(raw[5, rows, lanes(h)].astype(f32))
                pad[h, pl.ds(pl.multiple_of(32 + unit * UNIT, 32), UNIT), :] = mixed.astype(
                    bf16
                ).astype(f32)

    edge = sp_copy(pad.at[:, pl.ds(1024, 32), :], pad.at[:, pl.ds(0, 32), :], 1, ahead)
    along_y = [sp_copy(y_msg.at[y], y_msg.at[y], 1 + k, at_y(k)) for k in (1, 2, 3)]
    along_z = [sp_copy(z_msg.at[z], z_msg.at[z], 4 + k, at_z(k)) for k in (1, 2, 3)]
    swap = sp_copy(h_in.at[1 - core, core], h_in.at[1 - core, core], 8, partner)

    edge.start()

    pair_copy().wait()
    mine, mine_log = s_loc[core], a_loc[core, 0:1, :]
    other, other_log = unpack_state(p_recv)
    first = jnp.where(core == 0, mine, other)
    first_log = jnp.where(core == 0, mine_log, other_log)
    second = jnp.where(core == 0, other, mine)
    second_log = jnp.where(core == 0, other_log, mine_log)
    s_loc[core] = first
    a_loc[core] = jnp.broadcast_to(first_log, (8, 256))
    body, extra = pack_state(first * jnp.exp(second_log) + second, first_log + second_log)
    y_msg[y, 0:128, :] = body
    y_msg[y, 128:144, :] = extra
    for copy in along_y:
        copy.start()

    def filter_unit(unit):
        start = unit * UNIT + 2
        lane = lax.broadcasted_iota(jnp.int32, (UNIT, HEAD), 1)
        sums = jnp.zeros((UNIT, 1), f32)
        squares = jnp.zeros((UNIT, 1), f32)
        for g in range(4):
            total = jnp.zeros((UNIT, HEAD), f32)
            for j in range(31):
                total = total + taps[j : j + 1, lanes(g)] * pad[g, pl.ds(start + j, UNIT), :]
            filt[unit, :, lanes(g)] = total
            sums = sums + jnp.sum(total, axis=1, keepdims=True)
            squares = squares + jnp.sum(total * total, axis=1, keepdims=True)
        old = stat[0]
        stat[0] = jnp.where(lane == unit, sums, jnp.where(lane == unit + 8, squares, old))

    stat[0] = jnp.zeros((UNIT, HEAD), f32)

    @pl.loop(1, 5)
    def _(unit):
        filter_unit(unit)

    for copy in along_y:
        copy.wait()
    whole = jnp.zeros((128, 256), f32)
    whole_log = jnp.zeros((1, 256), f32)
    before = jnp.zeros((128, 256), f32)
    before_log = jnp.zeros((1, 256), f32)
    for k in range(4):
        state, log = unpack_state(y_msg.at[k])
        before = jnp.where(k == y, whole, before)
        before_log = jnp.where(k == y, whole_log, before_log)
        whole = whole * jnp.exp(log) + state
        whole_log = whole_log + log
    body, extra = pack_state(whole, whole_log)
    z_msg[z, 0:128, :] = body
    z_msg[z, 128:144, :] = extra
    for copy in along_z:
        copy.start()
    y_before, y_before_log = before, before_log
    s_loc[1 - core] = y_before
    a_loc[1 - core] = jnp.broadcast_to(y_before_log, (8, 256))

    @pl.loop(5, 8)
    def _(unit):
        filter_unit(unit)

    edge.wait()

    @pl.when(s == 0)
    def _():
        pad[:, 0:32, :] = jnp.zeros((4, 32, HEAD), f32)

    filter_unit(0)

    def stat_copy(k):
        return pltpu.make_async_remote_copy(
            src_ref=stat.at[0],
            dst_ref=stat.at[k],
            send_sem=st_send.at[k],
            recv_sem=st_recv.at[k],
            device_id={"tp": lax.rem(x + k, 4)},
            device_id_type=MESH,
        )

    stats = [stat_copy(k) for k in (1, 2, 3)]
    for copy in stats:
        copy.start()

    for copy in along_z:
        copy.wait()
    whole = jnp.zeros((128, 256), f32)
    before = jnp.zeros((128, 256), f32)
    for k in range(4):
        state, log = unpack_state(z_msg.at[k])
        before = jnp.where(k == z, whole, before)
        whole = whole * jnp.exp(log) + state
    chip_in = before * jnp.exp(a_loc[1 - core, 0:1, :]) + s_loc[1 - core]
    h_in[0, core] = chip_in
    h_in[1, core] = chip_in * jnp.exp(a_loc[core, 0:1, :]) + s_loc[core]
    swap.start()
    for copy in stats:
        copy.wait()
    stat[0] = (stat[0] + stat[1]) + (stat[2] + stat[3])
    loads[7].wait()
    loads[8].wait()
    swap.wait()

    state = jnp.concatenate([h_in[core, 0], h_in[core, 1]], axis=1)
    for u in range(8):
        h_unit[u] = state.astype(bf16)
        if u < 7:
            state = state * jnp.exp(a_unit[u, 0:1, :]) + s_unit[u]

    def scatter(k, target):
        return pltpu.make_async_remote_copy(
            src_ref=s_buf.at[k],
            dst_ref=r_buf.at[k],
            send_sem=rs_send.at[k],
            recv_sem=rs_recv.at[k],
            device_id={"tp": target},
            device_id_type=MESH,
        )

    reduce = [scatter(k, left if k in (0, 3, 4) else right) for k in range(6)]

    @pl.loop(0, 4)
    def _(step):
        unit_a = jnp.where(
            step == 0,
            2 * far,
            jnp.where(step == 1, 2 * right, jnp.where(step == 2, 2 * left, 2 * x)),
        )
        unit_b = jnp.where(
            step == 0,
            2 * far + 1,
            jnp.where(step == 1, 2 * left + 1, jnp.where(step == 2, 2 * right + 1, 2 * x + 1)),
        )

        @pl.loop(0, 2)
        def _(k):
            unit = jnp.where(k == 0, unit_a, unit_b)
            rows = pl.ds(pl.multiple_of(k * UNIT, UNIT), UNIT)
            lane = lax.broadcasted_iota(jnp.int32, (UNIT, HEAD), 1)
            totals = stat[0]
            sums = jnp.sum(jnp.where(lane == unit, totals, 0.0), axis=1, keepdims=True)
            squares = jnp.sum(jnp.where(lane == unit + 8, totals, 0.0), axis=1, keepdims=True)
            mean = sums * (1.0 / 2048)
            scale = lax.rsqrt(squares * (1.0 / 2048) - mean * mean + norm_epsilon)
            for h in range(4):
                rec = near[unit, :, lanes(h)] + lax.dot_general(
                    qfar[unit, :, lanes(h)],
                    h_unit[unit, :, lanes(h)],
                    NT,
                    preferred_element_type=f32,
                )
                power = jnp.mean(rec * rec, axis=1, keepdims=True)
                gate = rgate[unit, :, lanes(h)].astype(f32)
                rec = rec * lax.rsqrt(power + head_epsilon) * head_gain[...]
                o_in[rows, lanes(h)] = (rec * (gate * jax.nn.sigmoid(gate))).astype(bf16)
                conv = (filt[unit, :, lanes(h)] - mean) * scale * conv_gain[:, lanes(h)]
                o_in[rows, lanes(4 + h)] = (conv * jax.nn.sigmoid(conv)).astype(bf16)

        for c in range(4):
            cols = slice(c * 512, c * 512 + 512)
            part[:, cols] = dot(o_in[...], w_out[:, cols])

        for i in (0, 1):

            @pl.when(step == i)
            def _(i=i):
                s_buf[2 * i] = part[0:UNIT, :].astype(bf16)
                reduce[2 * i].start()
                s_buf[2 * i + 1] = part[UNIT : 2 * UNIT, :].astype(bf16)
                reduce[2 * i + 1].start()

        @pl.when(step == 2)
        def _():
            reduce[0].wait_recv()
            s_buf[4] = (part[0:UNIT, :] + r_buf[0].astype(f32)).astype(bf16)
            reduce[4].start()
            reduce[1].wait_recv()
            s_buf[5] = (part[UNIT : 2 * UNIT, :] + r_buf[1].astype(f32)).astype(bf16)
            reduce[5].start()

    for k in (2, 3, 4, 5):
        reduce[k].wait_recv()
    out[0:UNIT, :] = (
        part[0:UNIT, :] + r_buf[2].astype(f32) + r_buf[4].astype(f32)
    ).astype(bf16)
    out[UNIT : 2 * UNIT, :] = (
        part[UNIT : 2 * UNIT, :] + r_buf[3].astype(f32) + r_buf[5].astype(f32)
    ).astype(bf16)
    for copy in gather:
        copy.wait_send()
    for copy in reduce:
        copy.wait_send()


def on_device(
    tokens,
    norm_gain,
    w_query,
    w_forget,
    w_value,
    w_rgate,
    w_glu_value,
    w_glu_gate,
    forget_gap,
    decay_shift,
    head_gain,
    conv_taps,
    conv_gain,
    out_rec,
    out_conv,
):
    vmem = pl.BlockSpec(memory_space=pltpu.VMEM)
    hbm = pl.BlockSpec(memory_space=pl.ANY)
    dma = pltpu.SemaphoreType.DMA
    scratch = [
        pltpu.VMEM((256, 2048), bf16),
        pltpu.VMEM((8, 128, 2048), bf16),
        pltpu.VMEM((256, 2048), bf16),
        pltpu.VMEM((6, 2048, 512), bf16),
        pltpu.VMEM((1024, 2048), bf16),
        pltpu.VMEM((6, 256, 512), bf16),
        pltpu.VMEM((384, 512), bf16),
        pltpu.VMEM((2, 128, 512), f32),
        pltpu.VMEM((128, 512), f32),
        pltpu.VMEM((2, 128, 512), bf16),
        pltpu.VMEM((8, 128, 512), f32),
        pltpu.VMEM((8, 128, 512), bf16),
        pltpu.VMEM((8, 128, 512), bf16),
        pltpu.VMEM((4, 1056, 128), f32),
        pltpu.VMEM((8, 128, 512), f32),
        pltpu.VMEM((8, 128, 512), f32),
        pltpu.VMEM((8, 8, 512), f32),
        pltpu.VMEM((8, 128, 512), bf16),
        pltpu.VMEM((2, 128, 256), f32),
        pltpu.VMEM((2, 8, 256), f32),
        pltpu.VMEM((144, 256), bf16),
        pltpu.VMEM((144, 256), bf16),
        pltpu.VMEM((4, 144, 256), bf16),
        pltpu.VMEM((4, 144, 256), bf16),
        pltpu.VMEM((2, 2, 128, 256), f32),
        pltpu.VMEM((4, 128, 128), f32),
        pltpu.VMEM((256, 1024), bf16),
        pltpu.VMEM((256, 2048), f32),
        pltpu.VMEM((6, 128, 2048), bf16),
        pltpu.VMEM((6, 128, 2048), bf16),
        dma((9,)),
        dma((6,)),
        dma((6,)),
        dma((9,)),
        dma((9,)),
        dma((4,)),
        dma((4,)),
        dma((6,)),
        dma((6,)),
    ]
    return pl.pallas_call(
        kernel,
        out_shape=jax.ShapeDtypeStruct((256, 2048), bf16),
        in_specs=[hbm, vmem] + [hbm] * 6 + [vmem] * 5 + [hbm] * 2,
        out_specs=vmem,
        scratch_shapes=scratch,
        compiler_params=pltpu.CompilerParams(
            collective_id=0, has_side_effects=True, vmem_limit_bytes=62 * 1024 * 1024
        ),
    )(
        tokens,
        norm_gain[None],
        w_query,
        w_forget,
        w_value,
        w_rgate,
        w_glu_value,
        w_glu_gate,
        forget_gap[None],
        decay_shift,
        head_gain[None],
        conv_taps,
        conv_gain[None],
        out_rec,
        out_conv,
    )


def solution(mesh):
    placed = (
        P(("sp", "tp"), None),
        P(),
        P(None, "tp"),
        P(None, "tp"),
        P(None, "tp"),
        P(None, "tp"),
        P(None, "tp"),
        P(None, "tp"),
        P("tp"),
        P("sp", "tp"),
        P(),
        P(None, "tp"),
        P("tp"),
        P("tp", None),
        P("tp", None),
    )
    return jax.shard_map(
        on_device, mesh=mesh, in_specs=placed, out_specs=P(("sp", "tp"), None), check_vma=False
    )
```

```python
import jax
import jax.numpy as jnp
from jax import lax
from jax.experimental import pallas as pl
from jax.experimental.pallas import tpu as pltpu
from jax.sharding import PartitionSpec as P

MESH = pl.DeviceIdType.MESH
HEAD = 128
UNIT = 128
f32 = jnp.float32
bf16 = jnp.bfloat16
scope = jax.named_scope

norm_epsilon = 1e-05
head_epsilon = 1e-06

NT = (((1,), (1,)), ((), ()))
TN = (((0,), (0,)), ((), ()))


def dot(a, b):
    return jnp.dot(a, b, preferred_element_type=f32)


def split3(value):
    hi = value.astype(bf16)
    rest = value - hi.astype(f32)
    mid = rest.astype(bf16)
    low = (rest - mid.astype(f32)).astype(bf16)
    return hi, mid, low


def pack_state(state, log):
    hi, mid, low = split3(log)
    row = lax.broadcasted_iota(jnp.int32, (16, state.shape[1]), 0)
    extra = jnp.where(
        row == 0,
        hi.astype(f32),
        jnp.where(row == 1, mid.astype(f32), jnp.where(row == 2, low.astype(f32), 0.0)),
    )
    return state.astype(bf16), extra.astype(bf16)


def unpack_state(ref):
    state = ref[0:128, :].astype(f32)
    log = jnp.sum(ref[128:144, :].astype(f32), axis=0, keepdims=True)
    return state, log


def kernel(
    tokens,
    norm_gain_hbm,
    w_query,
    w_forget,
    w_value,
    w_rgate,
    w_glu_value,
    w_glu_gate,
    gap_hbm,
    shift_hbm,
    head_gain_hbm,
    taps_hbm,
    conv_gain_hbm,
    out_rec,
    out_conv,
    out,
    norm_gain,
    gap,
    shift,
    head_gain,
    taps,
    conv_gain,
    tok,
    xn,
    xp,
    w_in,
    w_rel,
    raw,
    hml,
    run,
    keys,
    kdec,
    near,
    qfar,
    rgate,
    pad,
    filt,
    s_unit,
    a_unit,
    h_unit,
    s_loc,
    a_loc,
    p_send,
    p_recv,
    y_msg,
    z_msg,
    h_in,
    stat,
    act,
    act_in,
    relay,
    acc,
    load_sem,
    ag_send,
    ag_recv,
    sp_send,
    sp_recv,
    st_send,
    st_recv,
    wx_send,
    wx_recv,
    wp_send,
    wp_recv,
    wc_send,
    wc_recv,
    aa_send,
    aa_recv,
):
    x = lax.axis_index("tp")
    s = lax.axis_index("sp")
    core = lax.rem(s, 2)
    chip = s // 2
    y = lax.rem(chip, 4)
    z = chip // 4

    def around(index, step):
        return lax.rem(index + step, 4)

    right, far, left = around(x, 1), around(x, 2), around(x, 3)
    behind = lax.rem(s + 31, 32)
    ahead = lax.rem(s + 1, 32)
    partner = chip * 2 + (1 - core)

    def at_y(k):
        return (z * 4 + around(y, k)) * 2 + core

    def at_z(k):
        return (around(z, k) * 4 + y) * 2 + core

    barrier = pltpu.get_barrier_semaphore()
    peers = [{"tp": right}, {"tp": left}, {"tp": far}, {"sp": partner}, {"sp": behind}]
    peers += [{"sp": at_y(k)} for k in (1, 2, 3)] + [{"sp": at_z(k)} for k in (1, 2, 3)]
    for peer in peers:
        pl.semaphore_signal(barrier, inc=1, device_id=peer, device_id_type=MESH)

    def remote(src, dst, send_sem, recv_sem, target):
        return pltpu.make_async_remote_copy(
            src_ref=src,
            dst_ref=dst,
            send_sem=send_sem,
            recv_sem=recv_sem,
            device_id=target,
            device_id_type=MESH,
        )

    pairs = [(tokens, tok), (norm_gain_hbm, norm_gain)]
    pairs += [
        (weight, w_in.at[k])
        for k, weight in enumerate(
            (w_forget, w_value, w_query, w_rgate, w_glu_value, w_glu_gate)
        )
    ]
    pairs += [
        (gap_hbm, gap),
        (shift_hbm, shift),
        (head_gain_hbm, head_gain),
        (taps_hbm, taps),
        (conv_gain_hbm, conv_gain),
        (out_rec, w_rel.at[0, 0]),
        (out_conv, w_rel.at[0, 1]),
    ]
    loads = [
        pltpu.make_async_copy(src, dst, load_sem.at[k]) for k, (src, dst) in enumerate(pairs)
    ]
    for load in loads:
        load.start()

    first_index, second_index = (y, z), (z, y)
    first_at, second_at = (at_y, at_z), (at_z, at_y)

    def slice_rows(p, j1, j2):
        return pl.ds(pl.multiple_of(16 * (core * 16 + 4 * j2 + j1), 16), 16)

    own_rows = [slice_rows(p, first_index[p], second_index[p]) for p in (0, 1)]
    weight_of = (out_rec, out_conv)

    def cross(k, p, slot, src, target):
        dst = w_rel.at[slot, p, own_rows[p]]
        return remote(src, dst, wx_send.at[k], wx_recv.at[k], {"tp": target})

    def own_slice(p):
        return weight_of[p].at[own_rows[p]]

    cross_out = [
        cross(0, 0, 3, own_slice(0), right),
        cross(1, 1, 3, own_slice(1), right),
        cross(2, 0, 1, own_slice(0), left),
        cross(3, 1, 1, own_slice(1), left),
        cross(4, 0, 2, w_rel.at[3, 0, own_rows[0]], right),
        cross(5, 1, 2, w_rel.at[1, 1, own_rows[1]], left),
    ]
    cross_in = cross_out

    def packet(p, j1, j2, half):
        cols = pl.ds(0, 2048) if half is None else pl.ds(1024 * half, 1024)
        return w_rel.at[pl.ds(1, 3), p, slice_rows(p, j1, j2), cols]

    def plane(p, k, j1, j2, half, target):
        ref = packet(p, j1, j2, half)
        return remote(ref, ref, wp_send.at[p, k], wp_recv.at[p, k], {"sp": target})

    plane_out, plane_in = [], []
    for p in (0, 1):
        i1, i2 = first_index[p], second_index[p]
        to1, to2 = first_at[p], second_at[p]
        sends = [
            (i1, i2, None, to1(1)),
            (i1, i2, None, to1(3)),
            (around(i1, 3), i2, 0, to1(1)),
            (around(i1, 1), i2, 1, to1(3)),
        ]
        comes = [
            (around(i1, 3), i2, None),
            (around(i1, 1), i2, None),
            (around(i1, 2), i2, 0),
            (around(i1, 2), i2, 1),
        ]
        for m in range(4):
            j1 = around(i1, m)
            sends += [
                (j1, i2, None, to2(1)),
                (j1, i2, None, to2(3)),
                (j1, around(i2, 3), 0, to2(1)),
                (j1, around(i2, 1), 1, to2(3)),
            ]
            comes += [
                (j1, around(i2, 3), None),
                (j1, around(i2, 1), None),
                (j1, around(i2, 2), 0),
                (j1, around(i2, 2), 1),
            ]
        plane_out.append([plane(p, k, *send) for k, send in enumerate(sends)])
        plane_in.append(
            [plane(p, k, *come, sends[k][3]) for k, come in enumerate(comes)]
        )

    def twin(p, n, owner):
        j2 = around(second_index[p], (0, 3, 1, 2)[n])
        rows = pl.ds(pl.multiple_of(256 * owner + 64 * j2, 64), 64)
        ref = w_rel.at[pl.ds(1, 3), p, rows]
        return remote(ref, ref, wc_send.at[p, n], wc_recv.at[p, n], {"sp": partner})

    twin_out = [[twin(p, n, core) for n in range(4)] for p in (0, 1)]
    twin_in = [[twin(p, n, 1 - core) for n in range(4)] for p in (0, 1)]

    def receive(k):
        for p in (1, 0):
            plane_in[p][k].wait_recv()

    def start(*ks):
        for k in ks:
            for p in (1, 0):
                plane_out[p][k].start()

    def weights_0():
        for k in (1, 2, 4, 5):
            cross_in[k].wait_recv()
        start(0, 1, 4, 5)

    def weights_1():
        receive(0)
        receive(1)
        start(2, 3)
        start(16, 17, 8, 9)

    def weights_2():
        receive(2)
        receive(3)
        start(12, 13)
        for p in (1, 0):
            twin_out[p][0].start()

    def weights_3(m):
        receive(4 + 4 * m)
        receive(5 + 4 * m)
        start(6 + 4 * m, 7 + 4 * m)

    def weights_4():
        for p in (1, 0):
            twin_out[p][1].start()
            twin_out[p][2].start()

    def weights_5():
        for m in (0, 3, 1, 2):
            receive(6 + 4 * m)
            receive(7 + 4 * m)
        for p in (1, 0):
            twin_out[p][3].start()

    def norm_rows(piece):
        for row in range(0, UNIT, 32):
            wide = tok[piece * UNIT + row : piece * UNIT + row + 32, :].astype(f32)
            mean = jnp.mean(wide, axis=1, keepdims=True)
            centred = wide - mean
            var = jnp.mean(centred * centred, axis=1, keepdims=True)
            value = centred * lax.rsqrt(var + norm_epsilon) * norm_gain[...]
            xn[2 * x + piece, row : row + 32, :] = value.astype(bf16)

    def send_unit(unit, k, target):
        return remote(
            xn.at[unit], xn.at[unit], ag_send.at[k], ag_recv.at[k], {"tp": target}
        )

    gather = [
        send_unit(2 * x, 0, right),
        send_unit(2 * x + 1, 1, right),
        send_unit(2 * left, 2, right),
        send_unit(2 * x + 1, 3, left),
        send_unit(2 * x, 4, left),
        send_unit(2 * right + 1, 5, left),
    ]
    arrive = [
        send_unit(2 * left, 0, right),
        send_unit(2 * left + 1, 1, right),
        send_unit(2 * far, 2, right),
        send_unit(2 * right + 1, 3, left),
        send_unit(2 * right, 4, left),
        send_unit(2 * far + 1, 5, left),
    ]
    with scope("w_barrier"):
        pl.semaphore_wait(barrier, len(peers))
    for k in range(4):
        cross_out[k].start()
    with scope("w_tok"):
        loads[0].wait()
        loads[1].wait()
    with scope("ln"):
        norm_rows(0)
        norm_rows(1)
    with scope("w_cross"):
        cross_in[0].wait_recv()
        cross_out[4].start()
        cross_in[3].wait_recv()
        cross_out[5].start()
    for k in (0, 3, 1, 4):
        gather[k].start()

    keep = lax.broadcasted_iota(jnp.int32, (UNIT, UNIT), 0) >= lax.broadcasted_iota(
        jnp.int32, (UNIT, UNIT), 1
    )
    ones_low = jnp.where(keep, 1.0, 0.0).astype(bf16)
    tri = jnp.concatenate([ones_low, ones_low, ones_low], axis=1)

    def lanes(h):
        return slice(h * HEAD, (h + 1) * HEAD)

    def units_of(step):
        unit_a = jnp.where(step == 0, 2 * x, jnp.where(step == 1, 2 * left, 2 * left + 1))
        unit_b = jnp.where(step == 0, 2 * x + 1, jnp.where(step == 1, 2 * right + 1, 2 * right))
        return unit_a, unit_b

    def project(*ks):
        for k in ks:
            raw[k] = dot(xp[...], w_in[k]).astype(bf16)

    def each_unit(unit_a, unit_b, body):
        @pl.loop(0, 2)
        def _(k):
            unit = jnp.where(k == 0, unit_a, unit_b)
            body(k, unit, pl.ds(pl.multiple_of(k * UNIT, UNIT), UNIT))

    def gates(k, unit, rows):
        for h in range(4):
            forget = raw[0, rows, lanes(h)].astype(f32)
            gate = gap[:, lanes(h)] * jax.nn.sigmoid(-forget)
            hi, mid, low = split3(jnp.log1p(-gate))
            hml[0:UNIT, lanes(h)] = hi
            hml[UNIT : 2 * UNIT, lanes(h)] = mid
            hml[2 * UNIT : 3 * UNIT, lanes(h)] = low
            keys[:, lanes(h)] = gate
        shifts = shift[:, pl.ds(pl.multiple_of(unit * UNIT, UNIT), UNIT)]
        shifts = jnp.concatenate(split3(shifts), axis=1)
        shift_run = lax.dot_general(tri, shifts, NT, preferred_element_type=f32)
        total = dot(tri, hml[...])
        for h in range(4):
            run_h = total[:, lanes(h)] + shift_run[:, h : h + 1]
            run[k, :, lanes(h)] = run_h
            centre = run_h[63:64, :]
            end = run_h[127:128, :]
            a_unit[unit, :, lanes(h)] = jnp.broadcast_to(end, (8, HEAD))
            decayed = keys[:, lanes(h)] * jnp.exp(centre - run_h)
            kdec[k, :, lanes(h)] = decayed.astype(bf16)
            ending = (decayed * jnp.exp(end - centre)).astype(bf16)
            s_unit[unit, :, lanes(h)] = lax.dot_general(
                raw[1, rows, lanes(h)], ending, TN, preferred_element_type=f32
            )

    def mix(k, unit, rows):
        for h in range(4):
            value = raw[4, rows, lanes(h)].astype(f32)
            mixed = value * jax.nn.sigmoid(raw[5, rows, lanes(h)].astype(f32))
            pad[h, pl.ds(pl.multiple_of(32 + unit * UNIT, 32), UNIT), :] = mixed.astype(
                bf16
            ).astype(f32)

    def scan(k, unit, rows):
        for h in range(4):
            run_h = run[k, :, lanes(h)]
            centre = run_h[63:64, :]
            query = raw[2, rows, lanes(h)].astype(f32)
            query = query * jax.nn.sigmoid(query) * jnp.exp(run_h - centre)
            qfar[unit, :, lanes(h)] = (query * jnp.exp(centre)).astype(bf16)
            scores = lax.dot_general(
                query.astype(bf16), kdec[k, :, lanes(h)], NT, preferred_element_type=f32
            )
            scores = jnp.where(keep, scores, 0.0).astype(bf16)
            near[unit, :, lanes(h)] = dot(scores, raw[1, rows, lanes(h)])
            rgate[unit, :, lanes(h)] = raw[3, rows, lanes(h)]

    @pl.loop(0, 3)
    def _(step):
        unit_a, unit_b = units_of(step)

        @pl.when(step == 0)
        def _():
            with scope("w_weights"):
                for k in range(2, 13):
                    loads[k].wait()

        @pl.when(step == 1)
        def _():
            with scope("w_w0"):
                weights_0()
            with scope("w_ag1"):
                arrive[0].wait_recv()
                gather[2].start()
                arrive[3].wait_recv()
                gather[5].start()

        @pl.when(step == 2)
        def _():
            with scope("w_w2"):
                weights_2()
            with scope("w_ag2"):
                arrive[1].wait_recv()
                arrive[4].wait_recv()

        with scope("proj_fv"):
            xp[0:UNIT, :] = xn[unit_a]
            xp[UNIT : 2 * UNIT, :] = xn[unit_b]
            project(0, 1)
        with scope("gates"):
            each_unit(unit_a, unit_b, gates)

        @pl.when(step == 1)
        def _():
            with scope("w_w1"):
                weights_1()

        @pl.when(step == 2)
        def _():
            with scope("w_w3_0"):
                weights_3(0)

        with scope("proj_rest"):
            project(2, 3, 4, 5)
        with scope("scan"):
            each_unit(unit_a, unit_b, mix)
            each_unit(unit_a, unit_b, scan)

    def sp_copy(src, dst, k, target):
        return remote(src, dst, sp_send.at[k], sp_recv.at[k], {"sp": target})

    pair = sp_copy(p_send, p_recv, 0, partner)
    edge = sp_copy(pad.at[:, pl.ds(1024, 32), :], pad.at[:, pl.ds(0, 32), :], 1, ahead)
    along_y = [sp_copy(y_msg.at[y], y_msg.at[y], 1 + k, at_y(k)) for k in (1, 2, 3)]
    along_z = [sp_copy(z_msg.at[z], z_msg.at[z], 4 + k, at_z(k)) for k in (1, 2, 3)]
    swap = sp_copy(h_in.at[1 - core, core], h_in.at[1 - core, core], 8, partner)

    with scope("w_w3_31"):
        weights_3(3)
        weights_3(1)
    with scope("w_ag3"):
        arrive[2].wait_recv()
        arrive[5].wait_recv()
    unit_a, unit_b = 2 * far, 2 * far + 1
    with scope("proj_fv"):
        xp[0:UNIT, :] = xn[unit_a]
        xp[UNIT : 2 * UNIT, :] = xn[unit_b]
        project(0, 1)
    with scope("gates"):
        each_unit(unit_a, unit_b, gates)
    with scope("combine"):
        state = s_unit[0]
        log = a_unit[0, 0:1, :]
        for u in range(1, 8):
            a_u = a_unit[u, 0:1, :]
            state = state * jnp.exp(a_u) + s_unit[u]
            log = log + a_u
        for half in range(2):
            part_of = slice(half * 256, half * 256 + 256)
            s_loc[half] = state[:, part_of]
            a_loc[half] = jnp.broadcast_to(log[:, part_of], (8, 256))
        body, extra = pack_state(s_loc[1 - core], a_loc[1 - core, 0:1, :])
        p_send[0:128, :] = body
        p_send[128:144, :] = extra
        pair.start()
    with scope("proj_glu"):
        project(4, 5)
        each_unit(unit_a, unit_b, mix)
        edge.start()

    with scope("w_pair"):
        pair.wait()
    mine, mine_log = s_loc[core], a_loc[core, 0:1, :]
    other, other_log = unpack_state(p_recv)
    first = jnp.where(core == 0, mine, other)
    first_log = jnp.where(core == 0, mine_log, other_log)
    second = jnp.where(core == 0, other, mine)
    second_log = jnp.where(core == 0, other_log, mine_log)
    s_loc[core] = first
    a_loc[core] = jnp.broadcast_to(first_log, (8, 256))
    body, extra = pack_state(first * jnp.exp(second_log) + second, first_log + second_log)
    y_msg[y, 0:128, :] = body
    y_msg[y, 128:144, :] = extra
    for copy in along_y:
        copy.start()

    with scope("proj_qr"):
        project(2, 3)
        each_unit(unit_a, unit_b, scan)

    def filter_unit(unit):
        begin = unit * UNIT + 2
        lane = lax.broadcasted_iota(jnp.int32, (UNIT, HEAD), 1)
        sums = jnp.zeros((UNIT, 1), f32)
        squares = jnp.zeros((UNIT, 1), f32)
        for g in range(4):
            total = jnp.zeros((UNIT, HEAD), f32)
            for j in range(31):
                total = total + taps[j : j + 1, lanes(g)] * pad[g, pl.ds(begin + j, UNIT), :]
            filt[unit, :, lanes(g)] = total
            sums = sums + jnp.sum(total, axis=1, keepdims=True)
            squares = squares + jnp.sum(total * total, axis=1, keepdims=True)
        old = stat[0]
        stat[0] = jnp.where(lane == unit, sums, jnp.where(lane == unit + 8, squares, old))

    stat[0] = jnp.zeros((UNIT, HEAD), f32)
    with scope("w_w3_2"):
        weights_3(2)
        weights_4()
    with scope("conv1"):

        @pl.loop(1, 5)
        def _(unit):
            filter_unit(unit)

    with scope("w_y"):
        for copy in along_y:
            copy.wait()
    whole = jnp.zeros((128, 256), f32)
    whole_log = jnp.zeros((1, 256), f32)
    before = jnp.zeros((128, 256), f32)
    before_log = jnp.zeros((1, 256), f32)
    for k in range(4):
        state, log = unpack_state(y_msg.at[k])
        before = jnp.where(k == y, whole, before)
        before_log = jnp.where(k == y, whole_log, before_log)
        whole = whole * jnp.exp(log) + state
        whole_log = whole_log + log
    body, extra = pack_state(whole, whole_log)
    z_msg[z, 0:128, :] = body
    z_msg[z, 128:144, :] = extra
    for copy in along_z:
        copy.start()
    s_loc[1 - core] = before
    a_loc[1 - core] = jnp.broadcast_to(before_log, (8, 256))

    with scope("conv2"):

        @pl.loop(5, 8)
        def _(unit):
            filter_unit(unit)

    with scope("w_edge"):
        edge.wait()

    @pl.when(s == 0)
    def _():
        pad[:, 0:32, :] = jnp.zeros((4, 32, HEAD), f32)

    with scope("conv0"):
        filter_unit(0)

    stats = [
        remote(stat.at[0], stat.at[k], st_send.at[k], st_recv.at[k], {"tp": around(x, k)})
        for k in (1, 2, 3)
    ]
    for copy in stats:
        copy.start()
    with scope("w_w5"):
        weights_5()
    with scope("w_stats"):
        for copy in stats:
            copy.wait()
    stat[0] = (stat[0] + stat[1]) + (stat[2] + stat[3])

    def exchange(p):
        def hop(k, src, dst, target):
            return remote(src, dst, aa_send.at[p, k], aa_recv.at[p, k], {"tp": target})

        low, high = pl.ds(0, UNIT), pl.ds(UNIT, UNIT)
        return [
            hop(0, act.at[2, p, low], relay.at[p, 0], right),
            hop(1, act.at[2, p, high], relay.at[p, 1], left),
            hop(2, act.at[1, p], act_in.at[3, p], right),
            hop(3, act.at[3, p], act_in.at[1, p], left),
            hop(4, relay.at[p, 0], act_in.at[2, p, low], right),
            hop(5, relay.at[p, 1], act_in.at[2, p, high], left),
        ]

    swaps = [exchange(0), exchange(1)]

    def each_row_block(o, body):
        @pl.loop(0, 2)
        def _(k):
            body(o, 2 * around(x, o) + k, pl.ds(pl.multiple_of(k * UNIT, UNIT), UNIT))

    def finish_conv(o, unit, rows):
        lane = lax.broadcasted_iota(jnp.int32, (UNIT, HEAD), 1)
        totals = stat[0]
        sums = jnp.sum(jnp.where(lane == unit, totals, 0.0), axis=1, keepdims=True)
        squares = jnp.sum(jnp.where(lane == unit + 8, totals, 0.0), axis=1, keepdims=True)
        mean = sums * (1.0 / 2048)
        scale = lax.rsqrt(squares * (1.0 / 2048) - mean * mean + norm_epsilon)
        for h in range(4):
            conv = (filt[unit, :, lanes(h)] - mean) * scale * conv_gain[:, lanes(h)]
            act[o, 1, rows, lanes(h)] = (conv * jax.nn.sigmoid(conv)).astype(bf16)

    def finish_rec(o, unit, rows):
        for h in range(4):
            rec = near[unit, :, lanes(h)] + lax.dot_general(
                qfar[unit, :, lanes(h)],
                h_unit[unit, :, lanes(h)],
                NT,
                preferred_element_type=f32,
            )
            power = jnp.mean(rec * rec, axis=1, keepdims=True)
            gate = rgate[unit, :, lanes(h)].astype(f32)
            rec = rec * lax.rsqrt(power + head_epsilon) * head_gain[...]
            act[o, 0, rows, lanes(h)] = (rec * (gate * jax.nn.sigmoid(gate))).astype(bf16)

    def finish_and_send(p, body):
        each_row_block(2, body)
        swaps[p][0].start()
        swaps[p][1].start()
        each_row_block(1, body)
        swaps[p][2].start()
        each_row_block(3, body)
        swaps[p][3].start()
        each_row_block(0, body)

    with scope("fin_conv"):
        finish_and_send(1, finish_conv)

    with scope("w_z"):
        for copy in along_z:
            copy.wait()
    whole = jnp.zeros((128, 256), f32)
    before = jnp.zeros((128, 256), f32)
    for k in range(4):
        state, log = unpack_state(z_msg.at[k])
        before = jnp.where(k == z, whole, before)
        whole = whole * jnp.exp(log) + state
    chip_in = before * jnp.exp(a_loc[1 - core, 0:1, :]) + s_loc[1 - core]
    h_in[0, core] = chip_in
    h_in[1, core] = chip_in * jnp.exp(a_loc[core, 0:1, :]) + s_loc[core]
    swap.start()
    with scope("w_relay_conv"):
        swaps[1][0].wait_recv()
        swaps[1][4].start()
        swaps[1][1].wait_recv()
        swaps[1][5].start()
    with scope("w_swap"):
        swap.wait()

    with scope("h_units"):
        state = jnp.concatenate([h_in[core, 0], h_in[core, 1]], axis=1)
        for u in range(8):
            h_unit[u] = state.astype(bf16)
            if u < 7:
                state = state * jnp.exp(a_unit[u, 0:1, :]) + s_unit[u]

    with scope("fin_rec"):
        finish_and_send(0, finish_rec)

    def add_product(k, p, begin):
        source = act.at[0, p] if k == 0 else act_in.at[k, p]
        for c in range(4):
            cols = slice(c * 512, c * 512 + 512)
            product = dot(source[...], w_rel[k, p, :, cols])
            acc[:, cols] = product if begin else acc[:, cols] + product

    with scope("w_twin"):
        loads[13].wait()
        loads[14].wait()
        for p in (1, 0):
            for n in range(4):
                twin_in[p][n].wait_recv()
    with scope("dot_conv"):
        add_product(0, 1, True)
        swaps[1][2].wait_recv()
        add_product(3, 1, False)
        swaps[1][3].wait_recv()
        add_product(1, 1, False)
    with scope("w_relay_rec"):
        swaps[0][0].wait_recv()
        swaps[0][4].start()
        swaps[0][1].wait_recv()
        swaps[0][5].start()
    with scope("dot_conv2"):
        swaps[1][4].wait_recv()
        swaps[1][5].wait_recv()
        add_product(2, 1, False)
        add_product(0, 0, False)
    with scope("dot_rec"):
        swaps[0][2].wait_recv()
        add_product(3, 0, False)
        swaps[0][3].wait_recv()
        add_product(1, 0, False)
    with scope("w_rec2"):
        swaps[0][4].wait_recv()
        swaps[0][5].wait_recv()
    with scope("dot_last"):
        for c in range(4):
            cols = slice(c * 512, c * 512 + 512)
            product = dot(act_in[2, 0], w_rel[2, 0, :, cols])
            out[:, cols] = (acc[:, cols] + product).astype(bf16)

    with scope("w_sends"):
        for copy in gather + cross_out + plane_out[0] + plane_out[1]:
            copy.wait_send()
        for copy in twin_out[0] + twin_out[1] + swaps[0] + swaps[1]:
            copy.wait_send()


def on_device(
    tokens,
    norm_gain,
    w_query,
    w_forget,
    w_value,
    w_rgate,
    w_glu_value,
    w_glu_gate,
    forget_gap,
    decay_shift,
    head_gain,
    conv_taps,
    conv_gain,
    out_rec,
    out_conv,
):
    vmem = pl.BlockSpec(memory_space=pltpu.VMEM)
    hbm = pl.BlockSpec(memory_space=pl.ANY)
    dma = pltpu.SemaphoreType.DMA
    scratch = [
        pltpu.VMEM((1, 2048), f32),
        pltpu.VMEM((1, 512), f32),
        pltpu.VMEM((4, 1024), f32),
        pltpu.VMEM((1, 128), f32),
        pltpu.VMEM((31, 512), f32),
        pltpu.VMEM((1, 512), f32),
        pltpu.VMEM((256, 2048), bf16),
        pltpu.VMEM((8, 128, 2048), bf16),
        pltpu.VMEM((256, 2048), bf16),
        pltpu.VMEM((6, 2048, 512), bf16),
        pltpu.VMEM((4, 2, 512, 2048), bf16),
        pltpu.VMEM((6, 256, 512), bf16),
        pltpu.VMEM((384, 512), bf16),
        pltpu.VMEM((2, 128, 512), f32),
        pltpu.VMEM((128, 512), f32),
        pltpu.VMEM((2, 128, 512), bf16),
        pltpu.VMEM((8, 128, 512), f32),
        pltpu.VMEM((8, 128, 512), bf16),
        pltpu.VMEM((8, 128, 512), bf16),
        pltpu.VMEM((4, 1056, 128), f32),
        pltpu.VMEM((8, 128, 512), f32),
        pltpu.VMEM((8, 128, 512), f32),
        pltpu.VMEM((8, 8, 512), f32),
        pltpu.VMEM((8, 128, 512), bf16),
        pltpu.VMEM((2, 128, 256), f32),
        pltpu.VMEM((2, 8, 256), f32),
        pltpu.VMEM((144, 256), bf16),
        pltpu.VMEM((144, 256), bf16),
        pltpu.VMEM((4, 144, 256), bf16),
        pltpu.VMEM((4, 144, 256), bf16),
        pltpu.VMEM((2, 2, 128, 256), f32),
        pltpu.VMEM((4, 128, 128), f32),
        pltpu.VMEM((4, 2, 256, 512), bf16),
        pltpu.VMEM((4, 2, 256, 512), bf16),
        pltpu.VMEM((2, 2, 128, 512), bf16),
        pltpu.VMEM((256, 2048), f32),
        dma((15,)),
        dma((6,)),
        dma((6,)),
        dma((9,)),
        dma((9,)),
        dma((4,)),
        dma((4,)),
        dma((6,)),
        dma((6,)),
        dma((2, 20)),
        dma((2, 20)),
        dma((2, 4)),
        dma((2, 4)),
        dma((2, 6)),
        dma((2, 6)),
    ]
    return pl.pallas_call(
        kernel,
        out_shape=jax.ShapeDtypeStruct((256, 2048), bf16),
        in_specs=[hbm] * 15,
        out_specs=vmem,
        scratch_shapes=scratch,
        compiler_params=pltpu.CompilerParams(
            collective_id=0, has_side_effects=True, vmem_limit_bytes=62 * 1024 * 1024
        ),
    )(
        tokens,
        norm_gain[None],
        w_query,
        w_forget,
        w_value,
        w_rgate,
        w_glu_value,
        w_glu_gate,
        forget_gap[None],
        decay_shift.T,
        head_gain[None],
        conv_taps,
        conv_gain[None],
        out_rec,
        out_conv,
    )


def solution(mesh):
    placed = (
        P(("sp", "tp"), None),
        P(),
        P(None, "tp"),
        P(None, "tp"),
        P(None, "tp"),
        P(None, "tp"),
        P(None, "tp"),
        P(None, "tp"),
        P("tp"),
        P("sp", "tp"),
        P(),
        P(None, "tp"),
        P("tp"),
        P("tp", None),
        P("tp", None),
    )
    return jax.shard_map(
        on_device, mesh=mesh, in_specs=placed, out_specs=P(("sp", "tp"), None), check_vma=False
    )
```

```python
import jax
import jax.numpy as jnp
from jax import lax
from jax.experimental import pallas as pl
from jax.experimental.pallas import tpu as pltpu
from jax.sharding import PartitionSpec as P

MESH = pl.DeviceIdType.MESH
HEAD = 128
UNIT = 128
f32 = jnp.float32
bf16 = jnp.bfloat16
scope = jax.named_scope

norm_epsilon = 1e-05
head_epsilon = 1e-06

NT = (((1,), (1,)), ((), ()))
TN = (((0,), (0,)), ((), ()))


def dot(a, b):
    return jnp.dot(a, b, preferred_element_type=f32)


def split3(value):
    hi = value.astype(bf16)
    rest = value - hi.astype(f32)
    mid = rest.astype(bf16)
    low = (rest - mid.astype(f32)).astype(bf16)
    return hi, mid, low


def pack_state(state, log):
    hi, mid, low = split3(log)
    row = lax.broadcasted_iota(jnp.int32, (16, state.shape[1]), 0)
    extra = jnp.where(
        row == 0,
        hi.astype(f32),
        jnp.where(row == 1, mid.astype(f32), jnp.where(row == 2, low.astype(f32), 0.0)),
    )
    return state.astype(bf16), extra.astype(bf16)


def unpack_state(ref):
    state = ref[0:128, :].astype(f32)
    log = jnp.sum(ref[128:144, :].astype(f32), axis=0, keepdims=True)
    return state, log


def kernel(
    tokens,
    norm_gain_hbm,
    w_query,
    w_forget,
    w_value,
    w_rgate,
    w_glu_value,
    w_glu_gate,
    gap_hbm,
    shift_hbm,
    head_gain_hbm,
    taps_hbm,
    conv_gain_hbm,
    out_rec,
    out_conv,
    out,
    norm_gain,
    gap,
    shift,
    head_gain,
    taps,
    conv_gain,
    tok,
    xn,
    xp,
    w_in,
    w_rel,
    raw,
    hml,
    run,
    keys,
    kdec,
    near,
    qfar,
    rgate,
    filt,
    s_unit,
    a_unit,
    h_unit,
    s_loc,
    a_loc,
    p_send,
    p_recv,
    y_msg,
    z_msg,
    h_in,
    act,
    act_in,
    relay,
    acc,
    w_own,
    mixed_in,
    c_in,
    c_pad,
    c_act,
    tg,
    load_sem,
    ag_send,
    ag_recv,
    sp_send,
    sp_recv,
    st_send,
    st_recv,
    wx_send,
    wx_recv,
    wp_send,
    wp_recv,
    wc_send,
    wc_recv,
    aa_send,
    aa_recv,
):
    x = lax.axis_index("tp")
    s = lax.axis_index("sp")
    core = lax.rem(s, 2)
    chip = s // 2
    y = lax.rem(chip, 4)
    z = chip // 4

    def around(index, step):
        return lax.rem(index + step, 4)

    right, far, left = around(x, 1), around(x, 2), around(x, 3)
    behind = lax.rem(s + 31, 32)
    ahead = lax.rem(s + 1, 32)
    partner = chip * 2 + (1 - core)

    def at_y(k):
        return (z * 4 + around(y, k)) * 2 + core

    def at_z(k):
        return (around(z, k) * 4 + y) * 2 + core

    barrier = pltpu.get_barrier_semaphore()
    peers = [{"tp": right}, {"tp": left}, {"tp": far}, {"sp": partner}, {"sp": behind}]
    peers += [{"sp": at_y(k)} for k in (1, 2, 3)] + [{"sp": at_z(k)} for k in (1, 2, 3)]
    for peer in peers:
        pl.semaphore_signal(barrier, inc=1, device_id=peer, device_id_type=MESH)

    def remote(src, dst, send_sem, recv_sem, target):
        return pltpu.make_async_remote_copy(
            src_ref=src,
            dst_ref=dst,
            send_sem=send_sem,
            recv_sem=recv_sem,
            device_id=target,
            device_id_type=MESH,
        )

    first_index, second_index = (y, z), (z, y)
    first_at, second_at = (at_y, at_z), (at_z, at_y)

    def slice_rows(p, j1, j2):
        return pl.ds(pl.multiple_of(16 * (core * 16 + 4 * j2 + j1), 16), 16)

    own_rows = [slice_rows(p, first_index[p], second_index[p]) for p in (0, 1)]
    weight_of = (out_rec, out_conv)

    own_loads = [
        pltpu.make_async_copy(weight_of[p].at[own_rows[p]], w_own.at[p], load_sem.at[15 + p])
        for p in (0, 1)
    ]
    pairs = [(tokens, tok), (norm_gain_hbm, norm_gain)]
    pairs += [
        (weight, w_in.at[k])
        for k, weight in enumerate(
            (w_forget, w_value, w_query, w_rgate, w_glu_value, w_glu_gate)
        )
    ]
    pairs += [
        (gap_hbm, gap),
        (shift_hbm, shift),
        (head_gain_hbm, head_gain),
        (taps_hbm, taps),
        (conv_gain_hbm, conv_gain),
        (out_rec, w_rel.at[0, 0]),
        (out_conv, w_rel.at[0, 1]),
    ]
    loads = [
        pltpu.make_async_copy(src, dst, load_sem.at[k]) for k, (src, dst) in enumerate(pairs)
    ]
    for load in own_loads + loads:
        load.start()

    def cross(k, p, slot, src, target):
        dst = w_rel.at[slot, p, own_rows[p]]
        return remote(src, dst, wx_send.at[k], wx_recv.at[k], {"tp": target})

    def own_slice(p):
        return w_own.at[p]

    cross_out = [
        cross(0, 0, 3, own_slice(0), right),
        cross(1, 1, 3, own_slice(1), right),
        cross(2, 0, 1, own_slice(0), left),
        cross(3, 1, 1, own_slice(1), left),
        cross(4, 0, 2, w_rel.at[3, 0, own_rows[0]], right),
        cross(5, 1, 2, w_rel.at[1, 1, own_rows[1]], left),
    ]
    cross_in = cross_out

    def packet(p, j1, j2, half):
        cols = pl.ds(0, 2048) if half is None else pl.ds(1024 * half, 1024)
        return w_rel.at[pl.ds(1, 3), p, slice_rows(p, j1, j2), cols]

    def plane(p, k, j1, j2, half, target):
        ref = packet(p, j1, j2, half)
        return remote(ref, ref, wp_send.at[p, k], wp_recv.at[p, k], {"sp": target})

    plane_out, plane_in = [], []
    for p in (0, 1):
        i1, i2 = first_index[p], second_index[p]
        to1, to2 = first_at[p], second_at[p]
        sends = [
            (i1, i2, None, to1(1)),
            (i1, i2, None, to1(3)),
            (around(i1, 3), i2, 0, to1(1)),
            (around(i1, 1), i2, 1, to1(3)),
        ]
        comes = [
            (around(i1, 3), i2, None),
            (around(i1, 1), i2, None),
            (around(i1, 2), i2, 0),
            (around(i1, 2), i2, 1),
        ]
        for m in range(4):
            j1 = around(i1, m)
            sends += [
                (j1, i2, None, to2(1)),
                (j1, i2, None, to2(3)),
                (j1, around(i2, 3), 0, to2(1)),
                (j1, around(i2, 1), 1, to2(3)),
            ]
            comes += [
                (j1, around(i2, 3), None),
                (j1, around(i2, 1), None),
                (j1, around(i2, 2), 0),
                (j1, around(i2, 2), 1),
            ]
        plane_out.append([plane(p, k, *send) for k, send in enumerate(sends)])
        plane_in.append(
            [plane(p, k, *come, sends[k][3]) for k, come in enumerate(comes)]
        )

    def twin(p, n, owner):
        j2 = around(second_index[p], (0, 3, 1, 2)[n])
        rows = pl.ds(pl.multiple_of(256 * owner + 64 * j2, 64), 64)
        ref = w_rel.at[pl.ds(1, 3), p, rows]
        return remote(ref, ref, wc_send.at[p, n], wc_recv.at[p, n], {"sp": partner})

    twin_out = [[twin(p, n, core) for n in range(4)] for p in (0, 1)]
    twin_in = [[twin(p, n, 1 - core) for n in range(4)] for p in (0, 1)]

    def receive(k):
        for p in (1, 0):
            plane_in[p][k].wait_recv()

    def start(*ks):
        for k in ks:
            for p in (1, 0):
                plane_out[p][k].start()

    def weights_0():
        for k in (1, 2, 4, 5):
            cross_in[k].wait_recv()
        start(0, 1, 4, 5)

    def weights_1():
        receive(0)
        receive(1)
        start(2, 3)
        start(16, 17, 8, 9)

    def weights_2():
        receive(2)
        receive(3)
        start(12, 13)
        for p in (1, 0):
            twin_out[p][0].start()

    def weights_3(m):
        receive(4 + 4 * m)
        receive(5 + 4 * m)
        start(6 + 4 * m, 7 + 4 * m)

    def weights_4():
        for p in (1, 0):
            twin_out[p][1].start()
            twin_out[p][2].start()

    def weights_5():
        for m in (0, 3, 1, 2):
            receive(6 + 4 * m)
            receive(7 + 4 * m)
        for p in (1, 0):
            twin_out[p][3].start()

    def norm_rows(piece):
        for row in range(0, UNIT, 32):
            wide = tok[piece * UNIT + row : piece * UNIT + row + 32, :].astype(f32)
            mean = jnp.mean(wide, axis=1, keepdims=True)
            centred = wide - mean
            var = jnp.mean(centred * centred, axis=1, keepdims=True)
            value = centred * lax.rsqrt(var + norm_epsilon) * norm_gain[...]
            xn[2 * x + piece, row : row + 32, :] = value.astype(bf16)

    def rows_copy(unit, begin, size, k, way):
        ref = xn.at[unit, pl.ds(begin, size)]
        target = {"tp": left if way else right}
        return remote(ref, ref, ag_send.at[way, k], ag_recv.at[way, k], target)

    parts = (
        ((1, 0, 32), (1, 32, 32), (1, 64, 64), (0, 0, 64), (0, 64, 64), (0, 0, 64), (1, 0, 64)),
        ((0, 64, 32), (0, 96, 32), (0, 0, 64), (1, 64, 64), (1, 0, 64), (0, 64, 64), (1, 64, 64)),
    )
    gather, arrive = [], []
    for way in (0, 1):
        source = left if way == 0 else right
        gather.append(
            [
                rows_copy(2 * (x if k < 5 else source) + u, begin, size, k, way)
                for k, (u, begin, size) in enumerate(parts[way])
            ]
        )
        arrive.append(
            [
                rows_copy(2 * (source if k < 5 else far) + u, begin, size, k, way)
                for k, (u, begin, size) in enumerate(parts[way])
            ]
        )

    def tokens_in(*ks):
        for k in ks:
            arrive[0][k].wait_recv()
            arrive[1][k].wait_recv()

    loads[0].wait()
    loads[1].wait()
    with scope("ln"):
        norm_rows(0)
        norm_rows(1)
    with scope("w_barrier"):
        pl.semaphore_wait(barrier, len(peers))
    for load in own_loads:
        load.wait()
    for k in range(4):
        cross_out[k].start()
    gather[0][0].start()
    gather[1][0].start()
    with scope("w_cross"):
        cross_in[0].wait_recv()
        cross_out[4].start()
        cross_in[3].wait_recv()
        cross_out[5].start()
    for k in range(1, 5):
        gather[0][k].start()
        gather[1][k].start()

    keep = lax.broadcasted_iota(jnp.int32, (UNIT, UNIT), 0) >= lax.broadcasted_iota(
        jnp.int32, (UNIT, UNIT), 1
    )
    ones_low = jnp.where(keep, 1.0, 0.0).astype(bf16)
    tri = jnp.concatenate([ones_low, ones_low, ones_low], axis=1)

    def lanes(h):
        return slice(h * HEAD, (h + 1) * HEAD)

    def units_of(step):
        unit_a = jnp.where(step == 0, 2 * x, jnp.where(step == 1, 2 * left + 1, 2 * left))
        unit_b = jnp.where(step == 0, 2 * x + 1, jnp.where(step == 1, 2 * right, 2 * right + 1))
        return unit_a, unit_b

    def project(*ks):
        for k in ks:
            raw[k] = dot(xp[...], w_in[k]).astype(bf16)

    def each_unit(unit_a, unit_b, body):
        for k, unit in enumerate((unit_a, unit_b)):
            body(k, unit, pl.ds(k * UNIT, UNIT))

    def gates(k, unit, rows):
        for h in range(4):
            forget = raw[0, rows, lanes(h)].astype(f32)
            gate = gap[:, lanes(h)] * jax.nn.sigmoid(-forget)
            hi, mid, low = split3(jnp.log1p(-gate))
            hml[k, 0:UNIT, lanes(h)] = hi
            hml[k, UNIT : 2 * UNIT, lanes(h)] = mid
            hml[k, 2 * UNIT : 3 * UNIT, lanes(h)] = low
            keys[k, :, lanes(h)] = gate
        shifts = shift[:, pl.ds(pl.multiple_of(unit * UNIT, UNIT), UNIT)]
        shifts = jnp.concatenate(split3(shifts), axis=1)
        shift_run = lax.dot_general(tri, shifts, NT, preferred_element_type=f32)
        total = dot(tri, hml[k])
        for h in range(4):
            run_h = total[:, lanes(h)] + shift_run[:, h : h + 1]
            run[k, :, lanes(h)] = run_h
            centre = run_h[63:64, :]
            end = run_h[127:128, :]
            a_unit[unit, :, lanes(h)] = jnp.broadcast_to(end, (8, HEAD))
            decayed = keys[k, :, lanes(h)] * jnp.exp(centre - run_h)
            kdec[k, :, lanes(h)] = decayed.astype(bf16)
            ending = (decayed * jnp.exp(end - centre)).astype(bf16)
            s_unit[unit, :, lanes(h)] = lax.dot_general(
                raw[1, rows, lanes(h)], ending, TN, preferred_element_type=f32
            )

    def mix(k, unit, rows):
        value = raw[4, rows, :].astype(f32)
        mixed = value * jax.nn.sigmoid(raw[5, rows, :].astype(f32))
        mixed_in[pl.ds(pl.multiple_of(32 + unit * UNIT, 32), UNIT), :] = mixed.astype(bf16)

    def scan(k, unit, rows):
        for h in range(4):
            run_h = run[k, :, lanes(h)]
            centre = run_h[63:64, :]
            query = raw[2, rows, lanes(h)].astype(f32)
            query = query * jax.nn.sigmoid(query) * jnp.exp(run_h - centre)
            qfar[unit, :, lanes(h)] = (query * jnp.exp(centre)).astype(bf16)
            scores = lax.dot_general(
                query.astype(bf16), kdec[k, :, lanes(h)], NT, preferred_element_type=f32
            )
            scores = jnp.where(keep, scores, 0.0).astype(bf16)
            near[unit, :, lanes(h)] = dot(scores, raw[1, rows, lanes(h)])
            rgate[unit, :, lanes(h)] = raw[3, rows, lanes(h)]

    def sp_copy(src, dst, k, target):
        return remote(src, dst, sp_send.at[k], sp_recv.at[k], {"sp": target})

    edge = sp_copy(mixed_in.at[pl.ds(1024, 32)], mixed_in.at[pl.ds(0, 32)], 1, ahead)

    def send_edge(owner):
        @pl.when(x == owner)
        def _():
            edge.start()

    def rows_of(o, begin, size):
        return mixed_in.at[pl.ds(pl.multiple_of(256 * around(x, o) + begin, 32), size)]

    def hop(p, k, src, dst, target):
        return remote(src, dst, aa_send.at[p, k], aa_recv.at[p, k], {"tp": target})

    low, high = pl.ds(0, UNIT), pl.ds(UNIT, UNIT)
    low_in, high_in = pl.ds(32, UNIT), pl.ds(32 + UNIT, UNIT)
    gated = [
        hop(1, 0, rows_of(2, 32, UNIT), relay.at[1, 0], left),
        hop(1, 1, rows_of(2, 32 + UNIT, UNIT), relay.at[1, 1], right),
        hop(1, 2, rows_of(1, 32, UNIT), c_in.at[3, low_in], right),
        hop(1, 3, rows_of(1, 32 + UNIT, UNIT), c_in.at[3, high_in], right),
        hop(1, 4, rows_of(3, 32, UNIT), c_in.at[1, low_in], left),
        hop(1, 5, rows_of(3, 32 + UNIT, UNIT), c_in.at[1, high_in], left),
        hop(1, 6, relay.at[1, 0], c_in.at[2, low_in], left),
        hop(1, 7, relay.at[1, 1], c_in.at[2, high_in], right),
    ]
    edges = [
        hop(1, 7 + o, rows_of(o, 0, 32), c_in.at[4 - o, pl.ds(0, 32)], {1: right, 2: far, 3: left}[o])
        for o in (1, 2, 3)
    ]
    acts = [
        hop(0, 0, act.at[2, low], relay.at[0, 0], left),
        hop(0, 1, act.at[2, high], relay.at[0, 1], right),
        hop(0, 2, act.at[1, low], act_in.at[3, low], right),
        hop(0, 3, act.at[1, high], act_in.at[3, high], right),
        hop(0, 4, act.at[3, low], act_in.at[1, low], left),
        hop(0, 5, act.at[3, high], act_in.at[1, high], left),
        hop(0, 6, relay.at[0, 0], act_in.at[2, low], left),
        hop(0, 7, relay.at[0, 1], act_in.at[2, high], right),
    ]
    filters = [
        remote(tg.at[0], tg.at[4 - j], st_send.at[j], st_recv.at[j], {"tp": around(x, j)})
        for j in (1, 2, 3)
    ]

    @pl.loop(0, 3)
    def _(step):
        unit_a, unit_b = units_of(step)

        @pl.when(step == 0)
        def _():
            with scope("w_weights"):
                for k in range(2, 13):
                    loads[k].wait()
            tg[0, 0:31, :] = taps[...]
            tg[0, 31:32, :] = conv_gain[...]

        @pl.when(step == 1)
        def _():
            with scope("w_ag1"):
                tokens_in(0, 1)
                gather[1][5].start()
                tokens_in(2)

        @pl.when(step == 2)
        def _():
            with scope("w_ag2"):
                tokens_in(3)
                gather[0][5].start()
                gather[0][6].start()
                gather[1][6].start()
                for copy in filters:
                    copy.start()
                tokens_in(4)
            with scope("w_w2"):
                weights_2()
                weights_3(0)

        with scope("proj_fv"):
            xp[0:UNIT, :] = xn[unit_a]
            xp[UNIT : 2 * UNIT, :] = xn[unit_b]
            project(0, 1)

        @pl.when(step == 1)
        def _():
            with scope("w_w1"):
                weights_1()

        with scope("gates"):
            each_unit(unit_a, unit_b, gates)

        with scope("proj_rest"):
            project(2, 3, 4, 5)

        @pl.when(step == 0)
        def _():
            with scope("w_w0"):
                weights_0()

        with scope("scan"):
            each_unit(unit_a, unit_b, mix)
            each_unit(unit_a, unit_b, scan)

        @pl.when(step == 0)
        def _():
            send_edge(3)

        @pl.when(step == 1)
        def _():
            send_edge(0)

        @pl.when(step == 2)
        def _():
            send_edge(2)

    unit_rows = pl.ds(0, UNIT)

    def project_unit(unit, *ks):
        for k in ks:
            raw[k, 0:UNIT, :] = dot(xn[unit], w_in[k]).astype(bf16)

    with scope("w_w3_31"):
        weights_3(3)
        weights_3(1)
    with scope("w_far_a"):
        tokens_in(5)
    with scope("far_a"):
        project_unit(2 * far, 0, 1)
        gates(0, 2 * far, unit_rows)
        project_unit(2 * far, 2, 3, 4, 5)
        mix(0, 2 * far, unit_rows)
        scan(0, 2 * far, unit_rows)
    with scope("w_far_b"):
        tokens_in(6)
    with scope("far_b"):
        project_unit(2 * far + 1, 0, 1)
        gates(0, 2 * far + 1, unit_rows)

    pair = sp_copy(p_send, p_recv, 0, partner)
    along_y = [
        [sp_copy(y_msg.at[y, hd], y_msg.at[y, hd], 1 + 3 * hd + k, at_y(k)) for k in (2, 1, 3)]
        for hd in (0, 1)
    ]
    along_z = [
        [sp_copy(z_msg.at[z, hd], z_msg.at[z, hd], 7 + 3 * hd + k, at_z(k)) for k in (2, 1, 3)]
        for hd in (0, 1)
    ]
    swap = sp_copy(h_in.at[1 - core, core], h_in.at[1 - core, core], 14, partner)

    with scope("combine"):
        state = s_unit[0]
        log = a_unit[0, 0:1, :]
        for u in range(1, 8):
            a_u = a_unit[u, 0:1, :]
            state = state * jnp.exp(a_u) + s_unit[u]
            log = log + a_u
        for half in range(2):
            part_of = slice(half * 256, half * 256 + 256)
            s_loc[half] = state[:, part_of]
            a_loc[half] = jnp.broadcast_to(log[:, part_of], (8, 256))
        body, extra = pack_state(s_loc[1 - core], a_loc[1 - core, 0:1, :])
        p_send[0:128, :] = body
        p_send[128:144, :] = extra
        pair.start()
    with scope("w_pair"):
        pair.wait()
    mine, mine_log = s_loc[core], a_loc[core, 0:1, :]
    other, other_log = unpack_state(p_recv)
    first = jnp.where(core == 0, mine, other)
    first_log = jnp.where(core == 0, mine_log, other_log)
    second = jnp.where(core == 0, other, mine)
    second_log = jnp.where(core == 0, other_log, mine_log)
    s_loc[core] = first
    a_loc[core] = jnp.broadcast_to(first_log, (8, 256))
    both = first * jnp.exp(second_log) + second
    both_log = first_log + second_log
    for hd in (0, 1):
        body, extra = pack_state(both[:, lanes(hd)], both_log[:, lanes(hd)])
        y_msg[y, hd, 0:128, :] = body
        y_msg[y, hd, 128:144, :] = extra
        for copy in along_y[hd]:
            copy.start()

    for k in (0, 2, 4, 5):
        gated[k].start()
    with scope("proj_glu"):
        project_unit(2 * far + 1, 4, 5)
        mix(0, 2 * far + 1, unit_rows)
        send_edge(1)
        gated[1].start()
        gated[3].start()

    with scope("w_w3_2"):
        weights_3(2)
        weights_4()

    with scope("proj_qr"):
        project_unit(2 * far + 1, 2, 3)
        scan(0, 2 * far + 1, unit_rows)

    def widen(k, begin, size):
        if k == 0:
            source = rows_of(0, begin, size)[...]
        else:
            source = c_in[k, begin : begin + size, :]
        for g in range(4):
            c_pad[4 * k + g, begin : begin + size, :] = source[:, lanes(g)].astype(f32)

    def filter_rows(k, u):
        for g in range(4):
            total = jnp.zeros((UNIT, HEAD), f32)
            for j in range(31):
                begin = u * UNIT + 2 + j
                total = (
                    total
                    + tg[k, j : j + 1, lanes(g)] * c_pad[4 * k + g, begin : begin + UNIT, :]
                )
            filt[u, :, lanes(4 * k + g)] = total

    with scope("w_edge"):
        edge.wait_recv()

        @pl.when(s == 0)
        def _():
            mixed_in[0:32, :] = jnp.zeros((32, 512), bf16)

    for copy in edges:
        copy.start()
    with scope("conv_0"):
        widen(0, 0, 288)
        filter_rows(0, 0)
        filter_rows(0, 1)

    for hd in (0, 1):
        with scope("w_y"):
            for copy in along_y[hd]:
                copy.wait()
        whole = jnp.zeros((128, HEAD), f32)
        whole_log = jnp.zeros((1, HEAD), f32)
        before = jnp.zeros((128, HEAD), f32)
        before_log = jnp.zeros((1, HEAD), f32)
        for k in range(4):
            state, log = unpack_state(y_msg.at[k, hd])
            before = jnp.where(k == y, whole, before)
            before_log = jnp.where(k == y, whole_log, before_log)
            whole = whole * jnp.exp(log) + state
            whole_log = whole_log + log
        body, extra = pack_state(whole, whole_log)
        z_msg[z, hd, 0:128, :] = body
        z_msg[z, hd, 128:144, :] = extra
        for copy in along_z[hd]:
            copy.start()
        s_loc[1 - core, :, lanes(hd)] = before
        a_loc[1 - core, :, lanes(hd)] = jnp.broadcast_to(before_log, (8, HEAD))

    with scope("w_relay_0"):
        gated[0].wait_recv()
        gated[6].start()
    with scope("w_filters"):
        for copy in filters:
            copy.wait()
    for hd in (0, 1):
        with scope("w_z"):
            for copy in along_z[hd]:
                copy.wait()
        whole = jnp.zeros((128, HEAD), f32)
        before = jnp.zeros((128, HEAD), f32)
        for k in range(4):
            state, log = unpack_state(z_msg.at[k, hd])
            before = jnp.where(k == z, whole, before)
            whole = whole * jnp.exp(log) + state
        chip_in = before * jnp.exp(a_loc[1 - core, 0:1, lanes(hd)]) + s_loc[1 - core, :, lanes(hd)]
        h_in[0, core, :, lanes(hd)] = chip_in
        h_in[1, core, :, lanes(hd)] = (
            chip_in * jnp.exp(a_loc[core, 0:1, lanes(hd)]) + s_loc[core, :, lanes(hd)]
        )
    swap.start()
    with scope("w_relay_1"):
        gated[1].wait_recv()
        gated[7].start()

    with scope("w_swap"):
        swap.wait()

    with scope("h_units"):
        state = jnp.concatenate([h_in[core, 0], h_in[core, 1]], axis=1)
        for u in range(8):
            h_unit[u] = state.astype(bf16)
            if u < 7:
                state = state * jnp.exp(a_unit[u, 0:1, :]) + s_unit[u]

    def finish_rec(o, k):
        unit = 2 * around(x, o) + k
        rows = slice(k * UNIT, k * UNIT + UNIT)
        for h in range(4):
            rec = near[unit, :, lanes(h)] + lax.dot_general(
                qfar[unit, :, lanes(h)],
                h_unit[unit, :, lanes(h)],
                NT,
                preferred_element_type=f32,
            )
            power = jnp.mean(rec * rec, axis=1, keepdims=True)
            gate = rgate[unit, :, lanes(h)].astype(f32)
            rec = rec * lax.rsqrt(power + head_epsilon) * head_gain[...]
            act[o, rows, lanes(h)] = (rec * (gate * jax.nn.sigmoid(gate))).astype(bf16)

    with scope("fin_rec"):
        finish_rec(2, 0)
        acts[0].start()
        finish_rec(2, 1)
        acts[1].start()
        finish_rec(1, 0)
        acts[2].start()
        finish_rec(3, 0)
        acts[4].start()
        finish_rec(1, 1)
        acts[3].start()
        finish_rec(3, 1)
        acts[5].start()
        finish_rec(0, 0)
        finish_rec(0, 1)

    with scope("w_w5"):
        weights_5()
    def add_product(source, k, p, begin):
        for c in range(4):
            cols = slice(c * 512, c * 512 + 512)
            product = dot(source, w_rel[k, p, :, cols])
            acc[:, cols] = product if begin else acc[:, cols] + product

    with scope("w_gated_1"):
        gated[4].wait_recv()
        gated[5].wait_recv()
    with scope("conv_1"):
        widen(1, 32, 256)
        filter_rows(1, 1)
    with scope("w_gated_3"):
        gated[2].wait_recv()
        gated[3].wait_recv()
    with scope("conv_3"):
        widen(3, 32, 256)
        filter_rows(3, 1)
    with scope("w_edges"):
        for copy in edges:
            copy.wait_recv()
    with scope("conv_13"):
        widen(1, 0, 32)
        filter_rows(1, 0)
        widen(3, 0, 32)
        filter_rows(3, 0)
    with scope("w_gated_2"):
        gated[6].wait_recv()
        gated[7].wait_recv()
    with scope("conv_2"):
        widen(2, 0, 288)
        filter_rows(2, 0)
        filter_rows(2, 1)
    with scope("w_relay_rec"):
        acts[0].wait_recv()
        acts[6].start()
        acts[1].wait_recv()
        acts[7].start()
    with scope("fin_conv"):
        for u in range(2):
            for row in range(0, UNIT, 32):
                rows = slice(row, row + 32)
                wide = filt[u, rows, :]
                mean = jnp.mean(wide, axis=1, keepdims=True)
                centred = wide - mean
                scale = lax.rsqrt(jnp.mean(centred * centred, axis=1, keepdims=True) + norm_epsilon)
                for k in range(4):
                    conv = filt[u, rows, k * 512 : k * 512 + 512] - mean
                    conv = conv * scale * tg[k, 31:32, :]
                    c_act[k, u * UNIT + row : u * UNIT + row + 32, :] = (
                        conv * jax.nn.sigmoid(conv)
                    ).astype(bf16)
    with scope("w_twin"):
        loads[13].wait()
        loads[14].wait()
        for p in (1, 0):
            for n in range(4):
                twin_in[p][n].wait_recv()
    with scope("dot_conv"):
        for k in range(4):
            add_product(c_act[k], k, 1, k == 0)
        add_product(act[0], 0, 0, False)
    with scope("dot_rec"):
        acts[2].wait_recv()
        acts[3].wait_recv()
        add_product(act_in[3], 3, 0, False)
        acts[4].wait_recv()
        acts[5].wait_recv()
        add_product(act_in[1], 1, 0, False)
    with scope("w_rec2"):
        acts[6].wait_recv()
        acts[7].wait_recv()
    with scope("dot_last"):
        for c in range(4):
            cols = slice(c * 512, c * 512 + 512)
            product = dot(act_in[2], w_rel[2, 0, :, cols])
            out[:, cols] = (acc[:, cols] + product).astype(bf16)

    with scope("w_sends"):
        edge.wait_send()
        for copy in gather[0] + gather[1] + cross_out + plane_out[0] + plane_out[1]:
            copy.wait_send()
        for copy in twin_out[0] + twin_out[1] + gated + edges + acts:
            copy.wait_send()


def on_device(
    tokens,
    norm_gain,
    w_query,
    w_forget,
    w_value,
    w_rgate,
    w_glu_value,
    w_glu_gate,
    forget_gap,
    decay_shift,
    head_gain,
    conv_taps,
    conv_gain,
    out_rec,
    out_conv,
):
    vmem = pl.BlockSpec(memory_space=pltpu.VMEM)
    hbm = pl.BlockSpec(memory_space=pl.ANY)
    dma = pltpu.SemaphoreType.DMA
    scratch = [
        pltpu.VMEM((1, 2048), f32),
        pltpu.VMEM((1, 512), f32),
        pltpu.VMEM((4, 1024), f32),
        pltpu.VMEM((1, 128), f32),
        pltpu.VMEM((31, 512), f32),
        pltpu.VMEM((1, 512), f32),
        pltpu.VMEM((256, 2048), bf16),
        pltpu.VMEM((8, 128, 2048), bf16),
        pltpu.VMEM((256, 2048), bf16),
        pltpu.VMEM((6, 2048, 512), bf16),
        pltpu.VMEM((4, 2, 512, 2048), bf16),
        pltpu.VMEM((6, 256, 512), bf16),
        pltpu.VMEM((2, 384, 512), bf16),
        pltpu.VMEM((2, 128, 512), f32),
        pltpu.VMEM((2, 128, 512), f32),
        pltpu.VMEM((2, 128, 512), bf16),
        pltpu.VMEM((8, 128, 512), f32),
        pltpu.VMEM((8, 128, 512), bf16),
        pltpu.VMEM((8, 128, 512), bf16),
        pltpu.VMEM((2, 128, 2048), f32),
        pltpu.VMEM((8, 128, 512), f32),
        pltpu.VMEM((8, 8, 512), f32),
        pltpu.VMEM((8, 128, 512), bf16),
        pltpu.VMEM((2, 128, 256), f32),
        pltpu.VMEM((2, 8, 256), f32),
        pltpu.VMEM((144, 256), bf16),
        pltpu.VMEM((144, 256), bf16),
        pltpu.VMEM((4, 2, 144, 128), bf16),
        pltpu.VMEM((4, 2, 144, 128), bf16),
        pltpu.VMEM((2, 2, 128, 256), f32),
        pltpu.VMEM((4, 256, 512), bf16),
        pltpu.VMEM((4, 256, 512), bf16),
        pltpu.VMEM((2, 2, 128, 512), bf16),
        pltpu.VMEM((256, 2048), f32),
        pltpu.VMEM((2, 16, 2048), bf16),
        pltpu.VMEM((1056, 512), bf16),
        pltpu.VMEM((4, 288, 512), bf16),
        pltpu.VMEM((16, 288, 128), f32),
        pltpu.VMEM((4, 256, 512), bf16),
        pltpu.VMEM((4, 32, 512), f32),
        dma((17,)),
        dma((2, 7)),
        dma((2, 7)),
        dma((15,)),
        dma((15,)),
        dma((4,)),
        dma((4,)),
        dma((6,)),
        dma((6,)),
        dma((2, 20)),
        dma((2, 20)),
        dma((2, 4)),
        dma((2, 4)),
        dma((2, 11)),
        dma((2, 11)),
    ]
    return pl.pallas_call(
        kernel,
        out_shape=pltpu.VMEM((256, 2048), bf16),
        in_specs=[hbm] * 15,
        out_specs=vmem,
        scratch_shapes=scratch,
        compiler_params=pltpu.CompilerParams(
            collective_id=0, has_side_effects=True, vmem_limit_bytes=60 * 1024 * 1024
        ),
    )(
        tokens,
        norm_gain[None],
        w_query,
        w_forget,
        w_value,
        w_rgate,
        w_glu_value,
        w_glu_gate,
        forget_gap[None],
        decay_shift.T,
        head_gain[None],
        conv_taps,
        conv_gain[None],
        out_rec,
        out_conv,
    )


def solution(mesh):
    placed = (
        P(("sp", "tp"), None),
        P(),
        P(None, "tp"),
        P(None, "tp"),
        P(None, "tp"),
        P(None, "tp"),
        P(None, "tp"),
        P(None, "tp"),
        P("tp"),
        P("sp", "tp"),
        P(),
        P(None, "tp"),
        P("tp"),
        P("tp", None),
        P("tp", None),
    )
    return jax.shard_map(
        on_device, mesh=mesh, in_specs=placed, out_specs=P(("sp", "tp"), None), check_vma=False
    )
```

```python
import jax
import jax.numpy as jnp
from jax import lax
from jax.experimental import pallas as pl
from jax.experimental.pallas import tpu as pltpu
from jax.sharding import PartitionSpec as P

MESH = pl.DeviceIdType.MESH
HEAD = 128
UNIT = 128
f32 = jnp.float32
bf16 = jnp.bfloat16
scope = jax.named_scope

norm_epsilon = 1e-05
head_epsilon = 1e-06

NT = (((1,), (1,)), ((), ()))
TN = (((0,), (0,)), ((), ()))


def dot(a, b):
    return jnp.dot(a, b, preferred_element_type=f32)


def split3(value):
    hi = value.astype(bf16)
    rest = value - hi.astype(f32)
    mid = rest.astype(bf16)
    low = (rest - mid.astype(f32)).astype(bf16)
    return hi, mid, low


def pack_state(state, log):
    hi, mid, low = split3(log)
    row = lax.broadcasted_iota(jnp.int32, (16, state.shape[1]), 0)
    extra = jnp.where(
        row == 0,
        hi.astype(f32),
        jnp.where(row == 1, mid.astype(f32), jnp.where(row == 2, low.astype(f32), 0.0)),
    )
    return state.astype(bf16), extra.astype(bf16)


def unpack_state(ref):
    state = ref[0:128, :].astype(f32)
    log = jnp.sum(ref[128:144, :].astype(f32), axis=0, keepdims=True)
    return state, log


def kernel(
    tokens,
    norm_gain_hbm,
    w_query,
    w_forget,
    w_value,
    w_rgate,
    w_glu_value,
    w_glu_gate,
    gap_hbm,
    shift_hbm,
    head_gain_hbm,
    taps_hbm,
    conv_gain_hbm,
    out_rec,
    out_conv,
    out,
    norm_gain,
    gap,
    shift,
    head_gain,
    taps,
    conv_gain,
    tok,
    xn,
    xp,
    w_in,
    w_rel,
    raw,
    hml,
    run,
    keys,
    kdec,
    near,
    qfar,
    rgate,
    filt,
    s_unit,
    a_unit,
    h_unit,
    s_loc,
    a_loc,
    p_send,
    p_recv,
    y_msg,
    z_msg,
    h_in,
    act,
    act_in,
    relay,
    acc,
    w_own,
    mixed_in,
    c_in,
    c_pad,
    c_act,
    tg,
    sems,
):
    x = lax.axis_index("tp")
    s = lax.axis_index("sp")
    core = lax.rem(s, 2)
    chip = s // 2
    y = lax.rem(chip, 4)
    z = chip // 4

    def around(index, step):
        return lax.rem(index + step, 4)

    right, far, left = around(x, 1), around(x, 2), around(x, 3)
    behind = lax.rem(s + 31, 32)
    ahead = lax.rem(s + 1, 32)
    partner = chip * 2 + (1 - core)

    def at_y(k):
        return (z * 4 + around(y, k)) * 2 + core

    def at_z(k):
        return (around(z, k) * 4 + y) * 2 + core

    barrier = pltpu.get_barrier_semaphore()
    peers = [{"tp": right}, {"tp": left}, {"tp": far}, {"sp": partner}, {"sp": behind}]
    peers += [{"sp": at_y(k)} for k in (1, 2, 3)] + [{"sp": at_z(k)} for k in (1, 2, 3)]
    for peer in peers:
        pl.semaphore_signal(barrier, inc=1, device_id=peer, device_id_type=MESH)

    def remote(src, dst, send_sem, recv_sem, target):
        return pltpu.make_async_remote_copy(
            src_ref=src,
            dst_ref=dst,
            send_sem=send_sem,
            recv_sem=recv_sem,
            device_id=target,
            device_id_type=MESH,
        )

    first_index, second_index = (y, z), (z, y)
    first_at, second_at = (at_y, at_z), (at_z, at_y)

    def slice_rows(p, j1, j2):
        return pl.ds(pl.multiple_of(16 * (core * 16 + 4 * j2 + j1), 16), 16)

    own_rows = [slice_rows(p, first_index[p], second_index[p]) for p in (0, 1)]
    weight_of = (out_rec, out_conv)

    def wait_for(ref, k):
        pltpu.make_async_copy(ref, ref, sems.at[k]).wait()

    own_loads = [
        pltpu.make_async_copy(weight_of[p].at[own_rows[p]], w_own.at[p], sems.at[9])
        for p in (0, 1)
    ]
    pairs = [(tokens, tok), (norm_gain_hbm, norm_gain)]
    pairs += [
        (weight, w_in.at[k])
        for k, weight in enumerate(
            (w_forget, w_value, w_query, w_rgate, w_glu_value, w_glu_gate)
        )
    ]
    pairs += [
        (gap_hbm, gap),
        (shift_hbm, shift),
        (head_gain_hbm, head_gain),
        (taps_hbm, taps),
        (conv_gain_hbm, conv_gain),
        (out_rec, w_rel.at[0, 0]),
        (out_conv, w_rel.at[0, 1]),
    ]
    loads = [
        pltpu.make_async_copy(src, dst, sems.at[(0, 1, 2, 2, 2, 2, 2, 2, 3, 4, 5, 6, 7, 8, 8)[k]])
        for k, (src, dst) in enumerate(pairs)
    ]
    for load in own_loads + loads:
        load.start()

    def cross(k, p, slot, src, target):
        dst = w_rel.at[slot, p, own_rows[p]]
        come = (17, 19, 19, 18, 19, 19)[k]
        return remote(src, dst, sems.at[16], sems.at[come], {"tp": target})

    def own_slice(p):
        return w_own.at[p]

    cross_out = [
        cross(0, 0, 3, own_slice(0), right),
        cross(1, 1, 3, own_slice(1), right),
        cross(2, 0, 1, own_slice(0), left),
        cross(3, 1, 1, own_slice(1), left),
        cross(4, 0, 2, w_rel.at[3, 0, own_rows[0]], right),
        cross(5, 1, 2, w_rel.at[1, 1, own_rows[1]], left),
    ]

    def packet(p, j1, j2, half):
        cols = pl.ds(0, 2048) if half is None else pl.ds(1024 * half, 1024)
        return w_rel.at[pl.ds(1, 3), p, slice_rows(p, j1, j2), cols]

    def plane(p, k, j1, j2, half, target):
        ref = packet(p, j1, j2, half)
        return remote(ref, ref, sems.at[20], sems.at[plane_sem[k]], {"sp": target})

    plane_sem = (21, 21, 22, 22, 23, 23, 26, 26, 24, 24, 26, 26, 25, 25, 26, 26, 24, 24, 26, 26)
    plane_out = []
    for p in (0, 1):
        i1, i2 = first_index[p], second_index[p]
        to1, to2 = first_at[p], second_at[p]
        sends = [
            (i1, i2, None, to1(1)),
            (i1, i2, None, to1(3)),
            (around(i1, 3), i2, 0, to1(1)),
            (around(i1, 1), i2, 1, to1(3)),
        ]
        for m in range(4):
            j1 = around(i1, m)
            sends += [
                (j1, i2, None, to2(1)),
                (j1, i2, None, to2(3)),
                (j1, around(i2, 3), 0, to2(1)),
                (j1, around(i2, 1), 1, to2(3)),
            ]
        plane_out.append([plane(p, k, *send) for k, send in enumerate(sends)])

    def twin(p, n, owner):
        j2 = around(second_index[p], (0, 3, 1, 2)[n])
        rows = pl.ds(pl.multiple_of(256 * owner + 64 * j2, 64), 64)
        ref = w_rel.at[pl.ds(1, 3), p, rows]
        return remote(ref, ref, sems.at[27], sems.at[28], {"sp": partner})

    twin_out = [[twin(p, n, core) for n in range(4)] for p in (0, 1)]

    def receive(k, rows):
        wait_for(w_rel.at[pl.ds(1, 3), 0, pl.ds(0, rows)], k)

    def start(*ks):
        for k in ks:
            for p in (1, 0):
                plane_out[p][k].start()

    def weights_0():
        wait_for(xn.at[0, pl.ds(0, 64)], 19)
        start(0, 1, 4, 5)

    def weights_1():
        receive(21, 64)
        start(2, 3)
        start(16, 17, 8, 9)

    def weights_2():
        receive(22, 32)
        start(12, 13)
        for p in (1, 0):
            twin_out[p][0].start()
        receive(23, 64)
        start(6, 7)

    def weights_3():
        receive(24, 128)
        start(18, 19, 10, 11)

    def weights_4():
        receive(25, 64)
        start(14, 15)
        for p in (1, 0):
            twin_out[p][1].start()
            twin_out[p][2].start()

    def weights_5():
        receive(26, 128)
        for p in (1, 0):
            twin_out[p][3].start()

    def norm_rows(piece):
        for row in range(0, UNIT, 32):
            wide = tok[piece * UNIT + row : piece * UNIT + row + 32, :].astype(f32)
            mean = jnp.mean(wide, axis=1, keepdims=True)
            centred = wide - mean
            var = jnp.mean(centred * centred, axis=1, keepdims=True)
            value = centred * lax.rsqrt(var + norm_epsilon) * norm_gain[...]
            xn[2 * x + piece, row : row + 32, :] = value.astype(bf16)

    def rows_copy(unit, begin, size, k, way):
        ref = xn.at[unit, pl.ds(begin, size)]
        target = {"tp": left if way else right}
        return remote(ref, ref, sems.at[10], sems.at[(11, 11, 11, 12, 13, 14, 15)[k]], target)

    parts = (
        ((1, 0, 32), (1, 32, 32), (1, 64, 64), (0, 0, 64), (0, 64, 64), (0, 0, 64), (1, 0, 64)),
        ((0, 64, 32), (0, 96, 32), (0, 0, 64), (1, 64, 64), (1, 0, 64), (0, 64, 64), (1, 64, 64)),
    )
    gather = []
    for way in (0, 1):
        source = left if way == 0 else right
        gather.append(
            [
                rows_copy(2 * (x if k < 5 else source) + u, begin, size, k, way)
                for k, (u, begin, size) in enumerate(parts[way])
            ]
        )

    def tokens_in(k):
        wait_for(xn.at[pl.ds(0, 2)] if k == 0 else xn.at[0], (11, None, None, 12, 13, 14, 15)[k])

    wait_for(w_own, 9)
    with scope("w_barrier"):
        pl.semaphore_wait(barrier, len(peers))
    for k in range(4):
        cross_out[k].start()
    with scope("w_tok"):
        loads[0].wait()
        loads[1].wait()
    with scope("ln"):
        norm_rows(0)
        norm_rows(1)
    gather[0][0].start()
    gather[1][0].start()
    with scope("w_cross"):
        cross_out[0].wait_recv()
        cross_out[4].start()
        cross_out[3].wait_recv()
        cross_out[5].start()
    for k in range(1, 5):
        gather[0][k].start()
        gather[1][k].start()

    keep = lax.broadcasted_iota(jnp.int32, (UNIT, UNIT), 0) >= lax.broadcasted_iota(
        jnp.int32, (UNIT, UNIT), 1
    )
    ones_low = jnp.where(keep, 1.0, 0.0).astype(bf16)
    tri = jnp.concatenate([ones_low, ones_low, ones_low], axis=1)

    def lanes(h):
        return slice(h * HEAD, (h + 1) * HEAD)

    def units_of(step):
        unit_a = jnp.where(step == 0, 2 * x, jnp.where(step == 1, 2 * left + 1, 2 * left))
        unit_b = jnp.where(step == 0, 2 * x + 1, jnp.where(step == 1, 2 * right, 2 * right + 1))
        return unit_a, unit_b

    def project(*ks):
        for k in ks:
            raw[k] = dot(xp[...], w_in[k]).astype(bf16)

    def each_unit(unit_a, unit_b, body):
        for k, unit in enumerate((unit_a, unit_b)):
            body(k, unit, pl.ds(k * UNIT, UNIT))

    def gates(k, unit, rows):
        for h in range(4):
            forget = raw[0, rows, lanes(h)].astype(f32)
            gate = gap[:, lanes(h)] * jax.nn.sigmoid(-forget)
            hi, mid, low = split3(jnp.log1p(-gate))
            hml[k, 0:UNIT, lanes(h)] = hi
            hml[k, UNIT : 2 * UNIT, lanes(h)] = mid
            hml[k, 2 * UNIT : 3 * UNIT, lanes(h)] = low
            keys[k, :, lanes(h)] = gate
        shifts = shift[:, pl.ds(pl.multiple_of(unit * UNIT, UNIT), UNIT)]
        shifts = jnp.concatenate(split3(shifts), axis=1)
        shift_run = lax.dot_general(tri, shifts, NT, preferred_element_type=f32)
        total = dot(tri, hml[k])
        for h in range(4):
            run_h = total[:, lanes(h)] + shift_run[:, h : h + 1]
            run[k, :, lanes(h)] = run_h
            centre = run_h[63:64, :]
            end = run_h[127:128, :]
            a_unit[unit, :, lanes(h)] = jnp.broadcast_to(end, (8, HEAD))
            decayed = keys[k, :, lanes(h)] * jnp.exp(centre - run_h)
            kdec[k, :, lanes(h)] = decayed.astype(bf16)
            ending = (decayed * jnp.exp(end - centre)).astype(bf16)
            s_unit[unit, :, lanes(h)] = lax.dot_general(
                raw[1, rows, lanes(h)], ending, TN, preferred_element_type=f32
            )

    def mix(k, unit, rows):
        value = raw[4, rows, :].astype(f32)
        mixed = value * jax.nn.sigmoid(raw[5, rows, :].astype(f32))
        mixed_in[pl.ds(pl.multiple_of(32 + unit * UNIT, 32), UNIT), :] = mixed.astype(bf16)

    def scan(k, unit, rows):
        for h in range(4):
            run_h = run[k, :, lanes(h)]
            centre = run_h[63:64, :]
            query = raw[2, rows, lanes(h)].astype(f32)
            query = query * jax.nn.sigmoid(query) * jnp.exp(run_h - centre)
            qfar[unit, :, lanes(h)] = (query * jnp.exp(centre)).astype(bf16)
            scores = lax.dot_general(
                query.astype(bf16), kdec[k, :, lanes(h)], NT, preferred_element_type=f32
            )
            scores = jnp.where(keep, scores, 0.0).astype(bf16)
            near[unit, :, lanes(h)] = dot(scores, raw[1, rows, lanes(h)])
            rgate[unit, :, lanes(h)] = raw[3, rows, lanes(h)]

    def sp_copy(ref, dst, send, come, target):
        return remote(ref, dst, sems.at[send], sems.at[come], {"sp": target})

    edge = sp_copy(mixed_in.at[pl.ds(1024, 32)], mixed_in.at[pl.ds(0, 32)], 31, 32, ahead)

    def send_edge(owner):
        @pl.when(x == owner)
        def _():
            edge.start()

    def rows_of(o, begin, size):
        return mixed_in.at[pl.ds(pl.multiple_of(256 * around(x, o) + begin, 32), size)]

    def hop(p, k, src, dst, target):
        send = (52, 44, 50)[p]
        come = 51 if p == 2 else (53, 45)[p] + (0, 1, 2, 2, 3, 3, 4, 4)[k]
        return remote(src, dst, sems.at[send], sems.at[come], {"tp": target})

    low, high = pl.ds(0, UNIT), pl.ds(UNIT, UNIT)
    low_in, high_in = pl.ds(32, UNIT), pl.ds(32 + UNIT, UNIT)
    gated = [
        hop(1, 0, rows_of(2, 32, UNIT), relay.at[1, 0], left),
        hop(1, 1, rows_of(2, 32 + UNIT, UNIT), relay.at[1, 1], right),
        hop(1, 2, rows_of(1, 32, UNIT), c_in.at[3, low_in], right),
        hop(1, 3, rows_of(1, 32 + UNIT, UNIT), c_in.at[3, high_in], right),
        hop(1, 4, rows_of(3, 32, UNIT), c_in.at[1, low_in], left),
        hop(1, 5, rows_of(3, 32 + UNIT, UNIT), c_in.at[1, high_in], left),
        hop(1, 6, relay.at[1, 0], c_in.at[2, low_in], left),
        hop(1, 7, relay.at[1, 1], c_in.at[2, high_in], right),
    ]
    edges = [
        hop(2, o, rows_of(o, 0, 32), c_in.at[4 - o, pl.ds(0, 32)], {1: right, 2: far, 3: left}[o])
        for o in (1, 2, 3)
    ]
    acts = [
        hop(0, 0, act.at[2, low], relay.at[0, 0], left),
        hop(0, 1, act.at[2, high], relay.at[0, 1], right),
        hop(0, 2, act.at[1, low], act_in.at[3, low], right),
        hop(0, 3, act.at[1, high], act_in.at[3, high], right),
        hop(0, 4, act.at[3, low], act_in.at[1, low], left),
        hop(0, 5, act.at[3, high], act_in.at[1, high], left),
        hop(0, 6, relay.at[0, 0], act_in.at[2, low], left),
        hop(0, 7, relay.at[0, 1], act_in.at[2, high], right),
    ]
    filters = [
        remote(tg.at[0], tg.at[4 - j], sems.at[42], sems.at[43], {"tp": around(x, j)})
        for j in (1, 2, 3)
    ]

    @pl.loop(0, 3)
    def _(step):
        unit_a, unit_b = units_of(step)

        @pl.when(step == 0)
        def _():
            with scope("w_weights"):
                wait_for(w_in, 2)
                for k in range(8, 13):
                    loads[k].wait()
            tg[0, 0:31, :] = taps[...]
            tg[0, 31:32, :] = conv_gain[...]

        @pl.when(step == 1)
        def _():
            with scope("w_ag1"):
                tokens_in(0)
                gather[1][5].start()

        @pl.when(step == 2)
        def _():
            with scope("w_ag2"):
                tokens_in(3)
                gather[0][5].start()
                gather[0][6].start()
                gather[1][6].start()
                for copy in filters:
                    copy.start()
                tokens_in(4)
            with scope("w_w2"):
                weights_2()

        with scope("proj_fv"):
            xp[0:UNIT, :] = xn[unit_a]
            xp[UNIT : 2 * UNIT, :] = xn[unit_b]
            project(0, 1)

        @pl.when(step == 1)
        def _():
            with scope("w_w1"):
                weights_1()

        with scope("gates"):
            each_unit(unit_a, unit_b, gates)

        with scope("proj_rest"):
            project(2, 3, 4, 5)

        @pl.when(step == 0)
        def _():
            with scope("w_w0"):
                weights_0()

        with scope("scan"):
            each_unit(unit_a, unit_b, mix)
            each_unit(unit_a, unit_b, scan)

        @pl.when(step == 0)
        def _():
            send_edge(3)

        @pl.when(step == 1)
        def _():
            send_edge(0)

        @pl.when(step == 2)
        def _():
            send_edge(2)

    unit_rows = pl.ds(0, UNIT)

    def project_unit(unit, *ks):
        for k in ks:
            raw[k, 0:UNIT, :] = dot(xn[unit], w_in[k]).astype(bf16)

    with scope("w_w3_31"):
        weights_3()
    with scope("w_far_a"):
        tokens_in(5)
    with scope("far_a"):
        project_unit(2 * far, 0, 1)
        gates(0, 2 * far, unit_rows)
        project_unit(2 * far, 2, 3, 4, 5)
        mix(0, 2 * far, unit_rows)
        scan(0, 2 * far, unit_rows)
    with scope("w_far_b"):
        tokens_in(6)
    with scope("far_b"):
        project_unit(2 * far + 1, 0, 1)
        gates(0, 2 * far + 1, unit_rows)

    pair = sp_copy(p_send, p_recv, 29, 30, partner)
    along_y = [
        [sp_copy(y_msg.at[y, hd], y_msg.at[y, hd], 33, 34 + hd, at_y(k)) for k in (2, 1, 3)]
        for hd in (0, 1)
    ]
    along_z = [
        [sp_copy(z_msg.at[z, hd], z_msg.at[z, hd], 36, 37 + hd, at_z(k)) for k in (2, 1, 3)]
        for hd in (0, 1)
    ]
    swap = [
        sp_copy(h_in.at[1 - core, core, hd], h_in.at[1 - core, core, hd], 39, 40 + hd, partner)
        for hd in (0, 1)
    ]

    with scope("combine"):
        state = s_unit[0]
        log = a_unit[0, 0:1, :]
        for u in range(1, 8):
            a_u = a_unit[u, 0:1, :]
            state = state * jnp.exp(a_u) + s_unit[u]
            log = log + a_u
        for half in range(2):
            part_of = slice(half * 256, half * 256 + 256)
            s_loc[half] = state[:, part_of]
            a_loc[half] = jnp.broadcast_to(log[:, part_of], (8, 256))
        body, extra = pack_state(s_loc[1 - core], a_loc[1 - core, 0:1, :])
        p_send[0:128, :] = body
        p_send[128:144, :] = extra
        pair.start()
    with scope("w_pair"):
        pair.wait_recv()
    mine, mine_log = s_loc[core], a_loc[core, 0:1, :]
    other, other_log = unpack_state(p_recv)
    first = jnp.where(core == 0, mine, other)
    first_log = jnp.where(core == 0, mine_log, other_log)
    second = jnp.where(core == 0, other, mine)
    second_log = jnp.where(core == 0, other_log, mine_log)
    s_loc[core] = first
    a_loc[core] = jnp.broadcast_to(first_log, (8, 256))
    both = first * jnp.exp(second_log) + second
    both_log = first_log + second_log
    for hd in (0, 1):
        body, extra = pack_state(both[:, lanes(hd)], both_log[:, lanes(hd)])
        y_msg[y, hd, 0:128, :] = body
        y_msg[y, hd, 128:144, :] = extra
        for copy in along_y[hd]:
            copy.start()

    for k in (0, 2, 4, 5):
        gated[k].start()
    with scope("proj_glu"):
        project_unit(2 * far + 1, 4, 5)
        mix(0, 2 * far + 1, unit_rows)
        send_edge(1)
        gated[1].start()
        gated[3].start()

    with scope("w_w3_2"):
        weights_4()

    with scope("proj_qr"):
        project_unit(2 * far + 1, 2, 3)
        scan(0, 2 * far + 1, unit_rows)

    def widen(k, begin, size):
        if k == 0:
            source = rows_of(0, begin, size)[...]
        else:
            source = c_in[k, begin : begin + size, :]
        for g in range(4):
            c_pad[4 * k + g, begin : begin + size, :] = source[:, lanes(g)].astype(f32)

    def filter_rows(k, u):
        for g in range(4):
            total = jnp.zeros((UNIT, HEAD), f32)
            for j in range(31):
                begin = u * UNIT + 2 + j
                total = (
                    total
                    + tg[k, j : j + 1, lanes(g)] * c_pad[4 * k + g, begin : begin + UNIT, :]
                )
            filt[u, :, lanes(4 * k + g)] = total

    with scope("w_edge"):
        edge.wait_recv()

        @pl.when(s == 0)
        def _():
            mixed_in[0:32, :] = jnp.zeros((32, 512), bf16)

    for copy in edges:
        copy.start()
    with scope("conv_0"):
        widen(0, 0, 288)
        filter_rows(0, 0)
        filter_rows(0, 1)

    for hd in (0, 1):
        with scope("w_y"):
            wait_for(y_msg.at[pl.ds(0, 3), hd], 34 + hd)
        whole = jnp.zeros((128, HEAD), f32)
        whole_log = jnp.zeros((1, HEAD), f32)
        before = jnp.zeros((128, HEAD), f32)
        before_log = jnp.zeros((1, HEAD), f32)
        for k in range(4):
            state, log = unpack_state(y_msg.at[k, hd])
            before = jnp.where(k == y, whole, before)
            before_log = jnp.where(k == y, whole_log, before_log)
            whole = whole * jnp.exp(log) + state
            whole_log = whole_log + log
        body, extra = pack_state(whole, whole_log)
        z_msg[z, hd, 0:128, :] = body
        z_msg[z, hd, 128:144, :] = extra
        for copy in along_z[hd]:
            copy.start()
        s_loc[1 - core, :, lanes(hd)] = before
        a_loc[1 - core, :, lanes(hd)] = jnp.broadcast_to(before_log, (8, HEAD))

    with scope("w_relay_0"):
        gated[0].wait_recv()
        gated[6].start()
    with scope("w_filters"):
        wait_for(tg.at[pl.ds(0, 3)], 43)
    for hd in (0, 1):
        with scope("w_z"):
            wait_for(z_msg.at[pl.ds(0, 3), hd], 37 + hd)
        whole = jnp.zeros((128, HEAD), f32)
        before = jnp.zeros((128, HEAD), f32)
        for k in range(4):
            state, log = unpack_state(z_msg.at[k, hd])
            before = jnp.where(k == z, whole, before)
            whole = whole * jnp.exp(log) + state
        chip_in = before * jnp.exp(a_loc[1 - core, 0:1, lanes(hd)]) + s_loc[1 - core, :, lanes(hd)]
        h_in[0, core, hd] = chip_in.astype(bf16)
        h_in[1, core, hd] = (
            chip_in * jnp.exp(a_loc[core, 0:1, lanes(hd)]) + s_loc[core, :, lanes(hd)]
        ).astype(bf16)
        swap[hd].start()
    with scope("w_relay_1"):
        gated[1].wait_recv()
        gated[7].start()

    with scope("w_swap"):
        swap[0].wait_recv()
        swap[1].wait_recv()

    with scope("h_units"):
        state = jnp.concatenate([h_in[core, h // 2, h % 2].astype(f32) for h in range(4)], axis=1)
        for u in range(8):
            h_unit[u] = state.astype(bf16)
            if u < 7:
                state = state * jnp.exp(a_unit[u, 0:1, :]) + s_unit[u]

    def finish_rec(o, k):
        unit = 2 * around(x, o) + k
        rows = slice(k * UNIT, k * UNIT + UNIT)
        for h in range(4):
            rec = near[unit, :, lanes(h)] + lax.dot_general(
                qfar[unit, :, lanes(h)],
                h_unit[unit, :, lanes(h)],
                NT,
                preferred_element_type=f32,
            )
            power = jnp.mean(rec * rec, axis=1, keepdims=True)
            gate = rgate[unit, :, lanes(h)].astype(f32)
            rec = rec * lax.rsqrt(power + head_epsilon) * head_gain[...]
            act[o, rows, lanes(h)] = (rec * (gate * jax.nn.sigmoid(gate))).astype(bf16)

    with scope("fin_rec"):
        finish_rec(2, 0)
        acts[0].start()
        finish_rec(2, 1)
        acts[1].start()
        finish_rec(1, 0)
        acts[2].start()
        finish_rec(3, 0)
        acts[4].start()
        finish_rec(1, 1)
        acts[3].start()
        finish_rec(3, 1)
        acts[5].start()
        finish_rec(0, 0)
        finish_rec(0, 1)

    with scope("w_w5"):
        weights_5()
    def add_product(source, k, p, begin):
        for c in range(4):
            cols = slice(c * 512, c * 512 + 512)
            product = dot(source, w_rel[k, p, :, cols])
            acc[:, cols] = product if begin else acc[:, cols] + product

    with scope("w_gated_1"):
        wait_for(c_in.at[1, pl.ds(32, 256)], 48)
    with scope("conv_1"):
        widen(1, 32, 256)
        filter_rows(1, 1)
    with scope("w_gated_3"):
        wait_for(c_in.at[3, pl.ds(32, 256)], 47)
    with scope("conv_3"):
        widen(3, 32, 256)
        filter_rows(3, 1)
    with scope("w_edges"):
        wait_for(mixed_in.at[pl.ds(0, 96)], 51)
    with scope("conv_13"):
        widen(1, 0, 32)
        filter_rows(1, 0)
        widen(3, 0, 32)
        filter_rows(3, 0)
    with scope("w_gated_2"):
        wait_for(c_in.at[2, pl.ds(32, 256)], 49)
    with scope("conv_2"):
        widen(2, 0, 288)
        filter_rows(2, 0)
        filter_rows(2, 1)
    with scope("w_relay_rec"):
        acts[0].wait_recv()
        acts[6].start()
        acts[1].wait_recv()
        acts[7].start()
    with scope("fin_conv"):
        for u in range(2):
            for row in range(0, UNIT, 32):
                rows = slice(row, row + 32)
                wide = filt[u, rows, :]
                mean = jnp.mean(wide, axis=1, keepdims=True)
                centred = wide - mean
                scale = lax.rsqrt(jnp.mean(centred * centred, axis=1, keepdims=True) + norm_epsilon)
                for k in range(4):
                    conv = filt[u, rows, k * 512 : k * 512 + 512] - mean
                    conv = conv * scale * tg[k, 31:32, :]
                    c_act[k, u * UNIT + row : u * UNIT + row + 32, :] = (
                        conv * jax.nn.sigmoid(conv)
                    ).astype(bf16)
    with scope("w_twin"):
        wait_for(w_rel.at[0], 8)
        wait_for(w_rel.at[pl.ds(1, 3), 0], 28)
    with scope("dot_conv"):
        for k in range(4):
            add_product(c_act[k], k, 1, k == 0)
        add_product(act[0], 0, 0, False)
    with scope("dot_rec"):
        wait_for(act_in.at[3], 55)
        add_product(act_in[3], 3, 0, False)
        wait_for(act_in.at[1], 56)
        add_product(act_in[1], 1, 0, False)
    with scope("w_rec2"):
        wait_for(act_in.at[2], 57)
    with scope("dot_last"):
        for c in range(4):
            cols = slice(c * 512, c * 512 + 512)
            product = dot(act_in[2], w_rel[2, 0, :, cols])
            out[:, cols] = (acc[:, cols] + product).astype(bf16)

    with scope("w_sends"):
        edge.wait_send()
        pair.wait_send()
        wait_for(xn.at[pl.ds(0, 6)], 10)
        wait_for(xn.at[0, pl.ds(0, 96)], 16)
        wait_for(w_rel.at[pl.ds(1, 3), 0, pl.ds(0, 480)], 20)
        wait_for(w_rel.at[pl.ds(1, 3), 0], 27)
        wait_for(y_msg.at[pl.ds(0, 3)], 33)
        wait_for(z_msg.at[pl.ds(0, 3)], 36)
        wait_for(h_in.at[0, 0], 39)
        wait_for(tg.at[pl.ds(0, 3)], 42)
        wait_for(act, 44)
        wait_for(mixed_in.at[pl.ds(0, 96)], 50)
        wait_for(act, 52)


def on_device(
    tokens,
    norm_gain,
    w_query,
    w_forget,
    w_value,
    w_rgate,
    w_glu_value,
    w_glu_gate,
    forget_gap,
    decay_shift,
    head_gain,
    conv_taps,
    conv_gain,
    out_rec,
    out_conv,
):
    vmem = pl.BlockSpec(memory_space=pltpu.VMEM)
    hbm = pl.BlockSpec(memory_space=pl.ANY)
    dma = pltpu.SemaphoreType.DMA
    scratch = [
        pltpu.VMEM((1, 2048), f32),
        pltpu.VMEM((1, 512), f32),
        pltpu.VMEM((4, 1024), f32),
        pltpu.VMEM((1, 128), f32),
        pltpu.VMEM((31, 512), f32),
        pltpu.VMEM((1, 512), f32),
        pltpu.VMEM((256, 2048), bf16),
        pltpu.VMEM((8, 128, 2048), bf16),
        pltpu.VMEM((256, 2048), bf16),
        pltpu.VMEM((6, 2048, 512), bf16),
        pltpu.VMEM((4, 2, 512, 2048), bf16),
        pltpu.VMEM((6, 256, 512), bf16),
        pltpu.VMEM((2, 384, 512), bf16),
        pltpu.VMEM((2, 128, 512), f32),
        pltpu.VMEM((2, 128, 512), f32),
        pltpu.VMEM((2, 128, 512), bf16),
        pltpu.VMEM((8, 128, 512), f32),
        pltpu.VMEM((8, 128, 512), bf16),
        pltpu.VMEM((8, 128, 512), bf16),
        pltpu.VMEM((2, 128, 2048), f32),
        pltpu.VMEM((8, 128, 512), f32),
        pltpu.VMEM((8, 8, 512), f32),
        pltpu.VMEM((8, 128, 512), bf16),
        pltpu.VMEM((2, 128, 256), f32),
        pltpu.VMEM((2, 8, 256), f32),
        pltpu.VMEM((144, 256), bf16),
        pltpu.VMEM((144, 256), bf16),
        pltpu.VMEM((4, 2, 144, 128), bf16),
        pltpu.VMEM((4, 2, 144, 128), bf16),
        pltpu.VMEM((2, 2, 2, 128, 128), bf16),
        pltpu.VMEM((4, 256, 512), bf16),
        pltpu.VMEM((4, 256, 512), bf16),
        pltpu.VMEM((2, 2, 128, 512), bf16),
        pltpu.VMEM((256, 2048), f32),
        pltpu.VMEM((2, 16, 2048), bf16),
        pltpu.VMEM((1056, 512), bf16),
        pltpu.VMEM((4, 288, 512), bf16),
        pltpu.VMEM((16, 288, 128), f32),
        pltpu.VMEM((4, 256, 512), bf16),
        pltpu.VMEM((4, 32, 512), f32),
        dma((58,)),
    ]
    return pl.pallas_call(
        kernel,
        out_shape=pltpu.VMEM((256, 2048), bf16),
        in_specs=[hbm] * 15,
        out_specs=vmem,
        scratch_shapes=scratch,
        compiler_params=pltpu.CompilerParams(
            collective_id=0, has_side_effects=True, vmem_limit_bytes=60 * 1024 * 1024
        ),
    )(
        tokens,
        norm_gain[None],
        w_query,
        w_forget,
        w_value,
        w_rgate,
        w_glu_value,
        w_glu_gate,
        forget_gap[None],
        decay_shift.T,
        head_gain[None],
        conv_taps,
        conv_gain[None],
        out_rec,
        out_conv,
    )


def solution(mesh):
    placed = (
        P(("sp", "tp"), None),
        P(),
        P(None, "tp"),
        P(None, "tp"),
        P(None, "tp"),
        P(None, "tp"),
        P(None, "tp"),
        P(None, "tp"),
        P("tp"),
        P("sp", "tp"),
        P(),
        P(None, "tp"),
        P("tp"),
        P("tp", None),
        P("tp", None),
    )
    return jax.shard_map(
        on_device, mesh=mesh, in_specs=placed, out_specs=P(("sp", "tp"), None), check_vma=False
    )
```

```python
import jax
import jax.numpy as jnp
from jax import lax
from jax.experimental import pallas as pl
from jax.experimental.pallas import tpu as pltpu
from jax.sharding import PartitionSpec as P

MESH = pl.DeviceIdType.MESH
HEAD = 128
UNIT = 128
f32 = jnp.float32
bf16 = jnp.bfloat16
scope = jax.named_scope

norm_epsilon = 1e-05
head_epsilon = 1e-06

NT = (((1,), (1,)), ((), ()))
TN = (((0,), (0,)), ((), ()))


def dot(a, b):
    return jnp.dot(a, b, preferred_element_type=f32)


def split3(value):
    hi = value.astype(bf16)
    rest = value - hi.astype(f32)
    mid = rest.astype(bf16)
    low = (rest - mid.astype(f32)).astype(bf16)
    return hi, mid, low


def pack_state(state, log):
    hi, mid, low = split3(log)
    row = lax.broadcasted_iota(jnp.int32, (16, state.shape[1]), 0)
    extra = jnp.where(
        row == 0,
        hi.astype(f32),
        jnp.where(row == 1, mid.astype(f32), jnp.where(row == 2, low.astype(f32), 0.0)),
    )
    return state.astype(bf16), extra.astype(bf16)


def unpack_state(ref):
    state = ref[0:128, :].astype(f32)
    log = jnp.sum(ref[128:144, :].astype(f32), axis=0, keepdims=True)
    return state, log


def kernel(
    tokens,
    norm_gain_hbm,
    w_query,
    w_forget,
    w_value,
    w_rgate,
    w_glu_value,
    w_glu_gate,
    gap_hbm,
    shift_hbm,
    head_gain_hbm,
    taps_hbm,
    conv_gain_hbm,
    out_rec,
    out_conv,
    out,
    norm_gain,
    gap,
    shift,
    head_gain,
    taps,
    conv_gain,
    tok,
    xn,
    xp,
    w_in,
    w_rel,
    raw,
    hml,
    run,
    keys,
    kdec,
    near,
    qfar,
    rgate,
    filt,
    s_unit,
    a_unit,
    h_unit,
    s_loc,
    a_loc,
    p_send,
    p_recv,
    y_msg,
    z_msg,
    h_in,
    act,
    act_in,
    relay,
    acc,
    w_own,
    mixed_in,
    c_in,
    c_pad,
    c_act,
    tg,
    sems,
):
    x = lax.axis_index("tp")
    s = lax.axis_index("sp")
    core = lax.rem(s, 2)
    chip = s // 2
    y = lax.rem(chip, 4)
    z = chip // 4

    def around(index, step):
        return lax.rem(index + step, 4)

    right, far, left = around(x, 1), around(x, 2), around(x, 3)
    behind = lax.rem(s + 31, 32)
    ahead = lax.rem(s + 1, 32)
    partner = chip * 2 + (1 - core)

    def at_y(k):
        return (z * 4 + around(y, k)) * 2 + core

    def at_z(k):
        return (around(z, k) * 4 + y) * 2 + core

    barrier = pltpu.get_barrier_semaphore()
    peers = [{"tp": right}, {"tp": left}, {"tp": far}, {"sp": partner}, {"sp": behind}]
    peers += [{"sp": at_y(k)} for k in (1, 2, 3)] + [{"sp": at_z(k)} for k in (1, 2, 3)]
    for peer in peers:
        pl.semaphore_signal(barrier, inc=1, device_id=peer, device_id_type=MESH)

    def remote(src, dst, send_sem, recv_sem, target):
        return pltpu.make_async_remote_copy(
            src_ref=src,
            dst_ref=dst,
            send_sem=send_sem,
            recv_sem=recv_sem,
            device_id=target,
            device_id_type=MESH,
        )

    first_index, second_index = (y, z), (z, y)
    first_at, second_at = (at_y, at_z), (at_z, at_y)

    def slice_rows(p, j1, j2):
        return pl.ds(pl.multiple_of(16 * (core * 16 + 4 * j2 + j1), 16), 16)

    own_rows = [slice_rows(p, first_index[p], second_index[p]) for p in (0, 1)]
    weight_of = (out_rec, out_conv)

    def wait_for(ref, k):
        pltpu.make_async_copy(ref, ref, sems.at[k]).wait()

    own_loads = [
        pltpu.make_async_copy(weight_of[p].at[own_rows[p]], w_own.at[p], sems.at[9])
        for p in (0, 1)
    ]
    pairs = [(tokens, tok), (norm_gain_hbm, norm_gain)]
    pairs += [
        (weight, w_in.at[k])
        for k, weight in enumerate(
            (w_forget, w_value, w_query, w_rgate, w_glu_value, w_glu_gate)
        )
    ]
    pairs += [
        (gap_hbm, gap),
        (shift_hbm, shift),
        (head_gain_hbm, head_gain),
        (taps_hbm, taps),
        (conv_gain_hbm, conv_gain),
        (out_rec, w_rel.at[0, 0]),
        (out_conv, w_rel.at[0, 1]),
    ]
    loads = [
        pltpu.make_async_copy(src, dst, sems.at[(0, 1, 2, 2, 2, 2, 2, 2, 3, 4, 5, 6, 7, 8, 8)[k]])
        for k, (src, dst) in enumerate(pairs)
    ]
    for load in own_loads + loads:
        load.start()

    def cross(k, p, slot, src, target):
        dst = w_rel.at[slot, p, own_rows[p]]
        come = (17, 19, 19, 18, 19, 19)[k]
        return remote(src, dst, sems.at[16], sems.at[come], {"tp": target})

    def own_slice(p):
        return w_own.at[p]

    cross_out = [
        cross(0, 0, 3, own_slice(0), right),
        cross(1, 1, 3, own_slice(1), right),
        cross(2, 0, 1, own_slice(0), left),
        cross(3, 1, 1, own_slice(1), left),
        cross(4, 0, 2, w_rel.at[3, 0, own_rows[0]], right),
        cross(5, 1, 2, w_rel.at[1, 1, own_rows[1]], left),
    ]

    def packet(p, j1, j2, half):
        cols = pl.ds(0, 2048) if half is None else pl.ds(1024 * half, 1024)
        return w_rel.at[pl.ds(1, 3), p, slice_rows(p, j1, j2), cols]

    def plane(p, k, j1, j2, half, target):
        ref = packet(p, j1, j2, half)
        return remote(ref, ref, sems.at[20], sems.at[plane_sem[k]], {"sp": target})

    plane_sem = (21, 21, 22, 22, 23, 23, 26, 26, 24, 24, 26, 26, 25, 25, 26, 26, 24, 24, 26, 26)
    plane_out = []
    for p in (0, 1):
        i1, i2 = first_index[p], second_index[p]
        to1, to2 = first_at[p], second_at[p]
        sends = [
            (i1, i2, None, to1(1)),
            (i1, i2, None, to1(3)),
            (around(i1, 3), i2, 0, to1(1)),
            (around(i1, 1), i2, 1, to1(3)),
        ]
        for m in range(4):
            j1 = around(i1, m)
            sends += [
                (j1, i2, None, to2(1)),
                (j1, i2, None, to2(3)),
                (j1, around(i2, 3), 0, to2(1)),
                (j1, around(i2, 1), 1, to2(3)),
            ]
        plane_out.append([plane(p, k, *send) for k, send in enumerate(sends)])

    def twin(p, n, owner):
        j2 = around(second_index[p], (0, 3, 1, 2)[n])
        rows = pl.ds(pl.multiple_of(256 * owner + 64 * j2, 64), 64)
        ref = w_rel.at[pl.ds(1, 3), p, rows]
        return remote(ref, ref, sems.at[27], sems.at[28], {"sp": partner})

    twin_out = [[twin(p, n, core) for n in range(4)] for p in (0, 1)]

    def receive(k, rows):
        wait_for(w_rel.at[pl.ds(1, 3), 0, pl.ds(0, rows)], k)

    def start(*ks):
        for k in ks:
            for p in (1, 0):
                plane_out[p][k].start()

    def weights_0():
        wait_for(xn.at[0, pl.ds(0, 64)], 19)
        start(0, 1, 4, 5)

    def weights_1():
        receive(21, 64)
        start(2, 3)
        start(16, 17, 8, 9)

    def weights_2():
        receive(22, 32)
        start(12, 13)
        for p in (1, 0):
            twin_out[p][0].start()
        receive(23, 64)
        start(6, 7)

    def weights_3():
        receive(24, 128)
        start(18, 19, 10, 11)

    def weights_4():
        receive(25, 64)
        start(14, 15)
        for p in (1, 0):
            twin_out[p][1].start()
            twin_out[p][2].start()

    def weights_5():
        receive(26, 128)
        for p in (1, 0):
            twin_out[p][3].start()

    def norm_rows(piece):
        for row in range(0, UNIT, 32):
            wide = tok[piece * UNIT + row : piece * UNIT + row + 32, :].astype(f32)
            mean = jnp.mean(wide, axis=1, keepdims=True)
            centred = wide - mean
            var = jnp.mean(centred * centred, axis=1, keepdims=True)
            value = centred * lax.rsqrt(var + norm_epsilon) * norm_gain[...]
            xn[2 * x + piece, row : row + 32, :] = value.astype(bf16)

    def rows_copy(unit, begin, size, k, way):
        ref = xn.at[unit, pl.ds(begin, size)]
        target = {"tp": left if way else right}
        return remote(ref, ref, sems.at[10], sems.at[(11, 11, 11, 12, 13, 14, 15)[k]], target)

    parts = (
        ((1, 0, 32), (1, 32, 32), (1, 64, 64), (0, 0, 64), (0, 64, 64), (0, 0, 64), (1, 0, 64)),
        ((0, 64, 32), (0, 96, 32), (0, 0, 64), (1, 64, 64), (1, 0, 64), (0, 64, 64), (1, 64, 64)),
    )
    gather = []
    for way in (0, 1):
        source = left if way == 0 else right
        gather.append(
            [
                rows_copy(2 * (x if k < 5 else source) + u, begin, size, k, way)
                for k, (u, begin, size) in enumerate(parts[way])
            ]
        )

    def tokens_in(k):
        wait_for(xn.at[pl.ds(0, 2)] if k == 0 else xn.at[0], (11, None, None, 12, 13, 14, 15)[k])

    wait_for(w_own, 9)
    with scope("w_barrier"):
        pl.semaphore_wait(barrier, len(peers))
    for k in range(4):
        cross_out[k].start()
    with scope("w_tok"):
        loads[0].wait()
        loads[1].wait()
    with scope("ln"):
        norm_rows(0)
        norm_rows(1)
    gather[0][0].start()
    gather[1][0].start()
    with scope("w_cross"):
        cross_out[0].wait_recv()
        cross_out[4].start()
        cross_out[3].wait_recv()
        cross_out[5].start()
    for k in range(1, 5):
        gather[0][k].start()
        gather[1][k].start()

    keep = lax.broadcasted_iota(jnp.int32, (UNIT, UNIT), 0) >= lax.broadcasted_iota(
        jnp.int32, (UNIT, UNIT), 1
    )
    ones_low = jnp.where(keep, 1.0, 0.0).astype(bf16)
    tri = jnp.concatenate([ones_low, ones_low, ones_low], axis=1)

    def lanes(h):
        return slice(h * HEAD, (h + 1) * HEAD)

    def units_of(step):
        unit_a = jnp.where(step == 0, 2 * x, jnp.where(step == 1, 2 * left + 1, 2 * left))
        unit_b = jnp.where(step == 0, 2 * x + 1, jnp.where(step == 1, 2 * right, 2 * right + 1))
        return unit_a, unit_b

    def project(*ks):
        for k in ks:
            raw[k] = dot(xp[...], w_in[k]).astype(bf16)

    def each_unit(unit_a, unit_b, body):
        for k, unit in enumerate((unit_a, unit_b)):
            body(k, unit, pl.ds(k * UNIT, UNIT))

    def gates(k, unit, rows):
        for h in range(4):
            forget = raw[0, rows, lanes(h)].astype(f32)
            gate = gap[:, lanes(h)] * jax.nn.sigmoid(-forget)
            hi, mid, low = split3(jnp.log1p(-gate))
            hml[k, 0:UNIT, lanes(h)] = hi
            hml[k, UNIT : 2 * UNIT, lanes(h)] = mid
            hml[k, 2 * UNIT : 3 * UNIT, lanes(h)] = low
            keys[k, :, lanes(h)] = gate
        shifts = shift[:, pl.ds(pl.multiple_of(unit * UNIT, UNIT), UNIT)]
        shifts = jnp.concatenate(split3(shifts), axis=1)
        shift_run = lax.dot_general(tri, shifts, NT, preferred_element_type=f32)
        total = dot(tri, hml[k])
        for h in range(4):
            run_h = total[:, lanes(h)] + shift_run[:, h : h + 1]
            run[k, :, lanes(h)] = run_h
            centre = run_h[63:64, :]
            end = run_h[127:128, :]
            a_unit[unit, :, lanes(h)] = jnp.broadcast_to(end, (8, HEAD))
            decayed = keys[k, :, lanes(h)] * jnp.exp(centre - run_h)
            kdec[k, :, lanes(h)] = decayed.astype(bf16)
            ending = (decayed * jnp.exp(end - centre)).astype(bf16)
            s_unit[unit, :, lanes(h)] = lax.dot_general(
                raw[1, rows, lanes(h)], ending, TN, preferred_element_type=f32
            )

    def mix(k, unit, rows):
        value = raw[4, rows, :].astype(f32)
        mixed = value * jax.nn.sigmoid(raw[5, rows, :].astype(f32))
        mixed_in[pl.ds(pl.multiple_of(32 + unit * UNIT, 32), UNIT), :] = mixed.astype(bf16)

    def scan(k, unit, rows):
        for h in range(4):
            run_h = run[k, :, lanes(h)]
            centre = run_h[63:64, :]
            query = raw[2, rows, lanes(h)].astype(f32)
            query = query * jax.nn.sigmoid(query) * jnp.exp(run_h - centre)
            qfar[unit, :, lanes(h)] = (query * jnp.exp(centre)).astype(bf16)
            scores = lax.dot_general(
                query.astype(bf16), kdec[k, :, lanes(h)], NT, preferred_element_type=f32
            )
            scores = jnp.where(keep, scores, 0.0).astype(bf16)
            near[unit, :, lanes(h)] = dot(scores, raw[1, rows, lanes(h)])
            rgate[unit, :, lanes(h)] = raw[3, rows, lanes(h)]

    def sp_copy(ref, dst, send, come, target):
        return remote(ref, dst, sems.at[send], sems.at[come], {"sp": target})

    edge = sp_copy(mixed_in.at[pl.ds(1024, 32)], mixed_in.at[pl.ds(0, 32)], 31, 32, ahead)

    def send_edge(owner):
        @pl.when(x == owner)
        def _():
            edge.start()

    def rows_of(o, begin, size):
        return mixed_in.at[pl.ds(pl.multiple_of(256 * around(x, o) + begin, 32), size)]

    def hop(p, k, src, dst, target):
        send = (52, 44, 50)[p]
        come = 51 if p == 2 else (53, 45)[p] + (0, 1, 2, 2, 3, 3, 4, 4)[k]
        return remote(src, dst, sems.at[send], sems.at[come], {"tp": target})

    low, high = pl.ds(0, UNIT), pl.ds(UNIT, UNIT)
    low_in, high_in = pl.ds(32, UNIT), pl.ds(32 + UNIT, UNIT)
    gated = [
        hop(1, 0, rows_of(2, 32, UNIT), relay.at[1, 0], left),
        hop(1, 1, rows_of(2, 32 + UNIT, UNIT), relay.at[1, 1], right),
        hop(1, 2, rows_of(1, 32, UNIT), c_in.at[3, low_in], right),
        hop(1, 3, rows_of(1, 32 + UNIT, UNIT), c_in.at[3, high_in], right),
        hop(1, 4, rows_of(3, 32, UNIT), c_in.at[1, low_in], left),
        hop(1, 5, rows_of(3, 32 + UNIT, UNIT), c_in.at[1, high_in], left),
        hop(1, 6, relay.at[1, 0], c_in.at[2, low_in], left),
        hop(1, 7, relay.at[1, 1], c_in.at[2, high_in], right),
    ]
    edges = [
        hop(2, o, rows_of(o, 0, 32), c_in.at[4 - o, pl.ds(0, 32)], {1: right, 2: far, 3: left}[o])
        for o in (1, 2, 3)
    ]
    acts = [
        hop(0, 0, act.at[2, low], relay.at[0, 0], left),
        hop(0, 1, act.at[2, high], relay.at[0, 1], right),
        hop(0, 2, act.at[1, low], act_in.at[3, low], right),
        hop(0, 3, act.at[1, high], act_in.at[3, high], right),
        hop(0, 4, act.at[3, low], act_in.at[1, low], left),
        hop(0, 5, act.at[3, high], act_in.at[1, high], left),
        hop(0, 6, relay.at[0, 0], act_in.at[2, low], left),
        hop(0, 7, relay.at[0, 1], act_in.at[2, high], right),
    ]
    filters = [
        remote(tg.at[0], tg.at[4 - j], sems.at[42], sems.at[43], {"tp": around(x, j)})
        for j in (1, 2, 3)
    ]

    @pl.loop(0, 3)
    def _(step):
        unit_a, unit_b = units_of(step)

        @pl.when(step == 0)
        def _():
            with scope("w_weights"):
                wait_for(w_in, 2)
                for k in range(8, 13):
                    loads[k].wait()
            tg[0, 0:31, :] = taps[...]
            tg[0, 31:32, :] = conv_gain[...]

        @pl.when(step == 1)
        def _():
            with scope("w_ag1"):
                tokens_in(0)
                gather[1][5].start()

        @pl.when(step == 2)
        def _():
            with scope("w_ag2"):
                tokens_in(3)
                gather[0][5].start()
                gather[0][6].start()
                gather[1][6].start()
                tokens_in(4)
            with scope("w_w2"):
                weights_2()

        with scope("proj_fv"):
            xp[0:UNIT, :] = xn[unit_a]
            xp[UNIT : 2 * UNIT, :] = xn[unit_b]
            project(0, 1)

        @pl.when(step == 1)
        def _():
            with scope("w_w1"):
                weights_1()

        with scope("gates"):
            each_unit(unit_a, unit_b, gates)

        with scope("proj_rest"):
            project(2, 3, 4, 5)

        @pl.when(step == 0)
        def _():
            with scope("w_w0"):
                weights_0()

        with scope("scan"):
            each_unit(unit_a, unit_b, mix)
            each_unit(unit_a, unit_b, scan)

        @pl.when(step == 0)
        def _():
            send_edge(3)

        @pl.when(step == 1)
        def _():
            send_edge(0)

        @pl.when(step == 2)
        def _():
            send_edge(2)

    unit_rows = pl.ds(0, UNIT)

    def project_unit(unit, *ks):
        for k in ks:
            raw[k, 0:UNIT, :] = dot(xn[unit], w_in[k]).astype(bf16)

    with scope("w_w3_31"):
        weights_3()
    with scope("w_far_a"):
        tokens_in(5)
    with scope("far_a"):
        project_unit(2 * far, 0, 1)
        gates(0, 2 * far, unit_rows)
        project_unit(2 * far, 2, 3, 4, 5)
        mix(0, 2 * far, unit_rows)
        scan(0, 2 * far, unit_rows)
    with scope("w_far_b"):
        tokens_in(6)
    for copy in filters:
        copy.start()
    for k in (0, 2, 5, 4):
        gated[k].start()
    with scope("far_b"):
        project_unit(2 * far + 1, 0, 1)
        gates(0, 2 * far + 1, unit_rows)

    pair = sp_copy(p_send, p_recv, 29, 30, partner)
    along_y = [
        [sp_copy(y_msg.at[y, hd], y_msg.at[y, hd], 33, 34 + hd, at_y(k)) for k in (2, 1, 3)]
        for hd in (0, 1)
    ]
    along_z = [
        [sp_copy(z_msg.at[z, hd], z_msg.at[z, hd], 36, 37 + hd, at_z(k)) for k in (2, 1, 3)]
        for hd in (0, 1)
    ]
    swap = [
        sp_copy(h_in.at[1 - core, core, hd], h_in.at[1 - core, core, hd], 39, 40 + hd, partner)
        for hd in (0, 1)
    ]

    with scope("combine"):
        state = s_unit[0]
        log = a_unit[0, 0:1, :]
        for u in range(1, 8):
            a_u = a_unit[u, 0:1, :]
            state = state * jnp.exp(a_u) + s_unit[u]
            log = log + a_u
        for half in range(2):
            part_of = slice(half * 256, half * 256 + 256)
            s_loc[half] = state[:, part_of]
            a_loc[half] = jnp.broadcast_to(log[:, part_of], (8, 256))
        body, extra = pack_state(s_loc[1 - core], a_loc[1 - core, 0:1, :])
        p_send[0:128, :] = body
        p_send[128:144, :] = extra
        pair.start()
    with scope("w_pair"):
        pair.wait_recv()
    mine, mine_log = s_loc[core], a_loc[core, 0:1, :]
    other, other_log = unpack_state(p_recv)
    first = jnp.where(core == 0, mine, other)
    first_log = jnp.where(core == 0, mine_log, other_log)
    second = jnp.where(core == 0, other, mine)
    second_log = jnp.where(core == 0, other_log, mine_log)
    s_loc[core] = first
    a_loc[core] = jnp.broadcast_to(first_log, (8, 256))
    both = first * jnp.exp(second_log) + second
    both_log = first_log + second_log
    for hd in (0, 1):
        body, extra = pack_state(both[:, lanes(hd)], both_log[:, lanes(hd)])
        y_msg[y, hd, 0:128, :] = body
        y_msg[y, hd, 128:144, :] = extra
        for copy in along_y[hd]:
            copy.start()

    with scope("proj_glu"):
        project_unit(2 * far + 1, 4, 5)
        mix(0, 2 * far + 1, unit_rows)
        send_edge(1)
        gated[1].start()
        gated[3].start()

    with scope("w_w3_2"):
        weights_4()

    with scope("proj_qr"):
        project_unit(2 * far + 1, 2, 3)
        scan(0, 2 * far + 1, unit_rows)

    def widen(k, begin, size):
        if k == 0:
            source = rows_of(0, begin, size)[...]
        else:
            source = c_in[k, begin : begin + size, :]
        for g in range(4):
            c_pad[4 * k + g, begin : begin + size, :] = source[:, lanes(g)].astype(f32)

    def filter_rows(k, u):
        for g in range(4):
            total = jnp.zeros((UNIT, HEAD), f32)
            for j in range(31):
                begin = u * UNIT + 2 + j
                total = (
                    total
                    + tg[k, j : j + 1, lanes(g)] * c_pad[4 * k + g, begin : begin + UNIT, :]
                )
            filt[u, :, lanes(4 * k + g)] = total

    for hd in (0, 1):
        with scope("w_y"):
            wait_for(y_msg.at[pl.ds(0, 3), hd], 34 + hd)
        whole = jnp.zeros((128, HEAD), f32)
        whole_log = jnp.zeros((1, HEAD), f32)
        before = jnp.zeros((128, HEAD), f32)
        before_log = jnp.zeros((1, HEAD), f32)
        for k in range(4):
            state, log = unpack_state(y_msg.at[k, hd])
            before = jnp.where(k == y, whole, before)
            before_log = jnp.where(k == y, whole_log, before_log)
            whole = whole * jnp.exp(log) + state
            whole_log = whole_log + log
        body, extra = pack_state(whole, whole_log)
        z_msg[z, hd, 0:128, :] = body
        z_msg[z, hd, 128:144, :] = extra
        for copy in along_z[hd]:
            copy.start()
        s_loc[1 - core, :, lanes(hd)] = before
        a_loc[1 - core, :, lanes(hd)] = jnp.broadcast_to(before_log, (8, HEAD))

    with scope("w_relay_0"):
        gated[0].wait_recv()
        gated[6].start()
    with scope("w_edge"):
        edge.wait_recv()

        @pl.when(s == 0)
        def _():
            mixed_in[0:32, :] = jnp.zeros((32, 512), bf16)

    for copy in edges:
        copy.start()
    with scope("conv_0"):
        widen(0, 0, 288)
        filter_rows(0, 0)
        filter_rows(0, 1)

    with scope("w_filters"):
        wait_for(tg.at[pl.ds(0, 3)], 43)
    for hd in (0, 1):
        with scope("w_z"):
            wait_for(z_msg.at[pl.ds(0, 3), hd], 37 + hd)
        whole = jnp.zeros((128, HEAD), f32)
        before = jnp.zeros((128, HEAD), f32)
        for k in range(4):
            state, log = unpack_state(z_msg.at[k, hd])
            before = jnp.where(k == z, whole, before)
            whole = whole * jnp.exp(log) + state
        chip_in = before * jnp.exp(a_loc[1 - core, 0:1, lanes(hd)]) + s_loc[1 - core, :, lanes(hd)]
        h_in[0, core, hd] = chip_in.astype(bf16)
        h_in[1, core, hd] = (
            chip_in * jnp.exp(a_loc[core, 0:1, lanes(hd)]) + s_loc[core, :, lanes(hd)]
        ).astype(bf16)
        swap[hd].start()
        if hd == 0:
            with scope("w_relay_1"):
                gated[1].wait_recv()
                gated[7].start()

    with scope("w_swap"):
        swap[0].wait_recv()
        swap[1].wait_recv()

    with scope("h_units"):
        state = jnp.concatenate([h_in[core, h // 2, h % 2].astype(f32) for h in range(4)], axis=1)
        for u in range(8):
            h_unit[u] = state.astype(bf16)
            if u < 7:
                state = state * jnp.exp(a_unit[u, 0:1, :]) + s_unit[u]

    def finish_rec(o, k):
        unit = 2 * around(x, o) + k
        rows = slice(k * UNIT, k * UNIT + UNIT)
        for h in range(4):
            rec = near[unit, :, lanes(h)] + lax.dot_general(
                qfar[unit, :, lanes(h)],
                h_unit[unit, :, lanes(h)],
                NT,
                preferred_element_type=f32,
            )
            power = jnp.mean(rec * rec, axis=1, keepdims=True)
            gate = rgate[unit, :, lanes(h)].astype(f32)
            rec = rec * lax.rsqrt(power + head_epsilon) * head_gain[...]
            act[o, rows, lanes(h)] = (rec * (gate * jax.nn.sigmoid(gate))).astype(bf16)

    with scope("fin_rec"):
        finish_rec(2, 0)
        acts[0].start()
        finish_rec(2, 1)
        acts[1].start()
        finish_rec(1, 0)
        acts[2].start()
        finish_rec(3, 0)
        acts[4].start()
        finish_rec(1, 1)
        acts[3].start()
        finish_rec(3, 1)
        acts[5].start()
        finish_rec(0, 0)
        finish_rec(0, 1)

    with scope("w_w5"):
        weights_5()
    def add_product(source, k, p, begin):
        for c in range(4):
            cols = slice(c * 512, c * 512 + 512)
            product = dot(source, w_rel[k, p, :, cols])
            acc[:, cols] = product if begin else acc[:, cols] + product

    with scope("w_gated_1"):
        wait_for(c_in.at[1, pl.ds(32, 256)], 48)
    with scope("conv_1"):
        widen(1, 32, 256)
        filter_rows(1, 1)
    with scope("w_gated_3"):
        wait_for(c_in.at[3, pl.ds(32, 256)], 47)
    with scope("conv_3"):
        widen(3, 32, 256)
        filter_rows(3, 1)
    with scope("w_edges"):
        wait_for(mixed_in.at[pl.ds(0, 96)], 51)
    with scope("conv_13"):
        widen(1, 0, 32)
        filter_rows(1, 0)
        widen(3, 0, 32)
        filter_rows(3, 0)
    with scope("w_gated_2"):
        wait_for(c_in.at[2, pl.ds(32, 256)], 49)
    with scope("conv_2"):
        widen(2, 0, 288)
        filter_rows(2, 0)
        filter_rows(2, 1)
    with scope("w_relay_rec"):
        acts[0].wait_recv()
        acts[6].start()
        acts[1].wait_recv()
        acts[7].start()
    with scope("fin_conv"):
        for u in range(2):
            for row in range(0, UNIT, 32):
                rows = slice(row, row + 32)
                wide = filt[u, rows, :]
                mean = jnp.mean(wide, axis=1, keepdims=True)
                centred = wide - mean
                scale = lax.rsqrt(jnp.mean(centred * centred, axis=1, keepdims=True) + norm_epsilon)
                for k in range(4):
                    conv = filt[u, rows, k * 512 : k * 512 + 512] - mean
                    conv = conv * scale * tg[k, 31:32, :]
                    c_act[k, u * UNIT + row : u * UNIT + row + 32, :] = (
                        conv * jax.nn.sigmoid(conv)
                    ).astype(bf16)
    with scope("w_twin"):
        wait_for(w_rel.at[0], 8)
        wait_for(w_rel.at[pl.ds(1, 3), 0], 28)
    with scope("dot_conv"):
        for k in range(4):
            add_product(c_act[k], k, 1, k == 0)
        add_product(act[0], 0, 0, False)
    with scope("dot_rec"):
        wait_for(act_in.at[3], 55)
        add_product(act_in[3], 3, 0, False)
        wait_for(act_in.at[1], 56)
        add_product(act_in[1], 1, 0, False)
    with scope("w_rec2"):
        wait_for(act_in.at[2], 57)
    with scope("dot_last"):
        for c in range(4):
            cols = slice(c * 512, c * 512 + 512)
            product = dot(act_in[2], w_rel[2, 0, :, cols])
            out[:, cols] = (acc[:, cols] + product).astype(bf16)

    with scope("w_sends"):
        edge.wait_send()
        pair.wait_send()
        wait_for(xn.at[pl.ds(0, 6)], 10)
        wait_for(xn.at[0, pl.ds(0, 96)], 16)
        wait_for(w_rel.at[pl.ds(1, 3), 0, pl.ds(0, 480)], 20)
        wait_for(w_rel.at[pl.ds(1, 3), 0], 27)
        wait_for(y_msg.at[pl.ds(0, 3)], 33)
        wait_for(z_msg.at[pl.ds(0, 3)], 36)
        wait_for(h_in.at[0, 0], 39)
        wait_for(tg.at[pl.ds(0, 3)], 42)
        wait_for(act, 44)
        wait_for(mixed_in.at[pl.ds(0, 96)], 50)
        wait_for(act, 52)


def on_device(
    tokens,
    norm_gain,
    w_query,
    w_forget,
    w_value,
    w_rgate,
    w_glu_value,
    w_glu_gate,
    forget_gap,
    decay_shift,
    head_gain,
    conv_taps,
    conv_gain,
    out_rec,
    out_conv,
):
    vmem = pl.BlockSpec(memory_space=pltpu.VMEM)
    hbm = pl.BlockSpec(memory_space=pl.ANY)
    dma = pltpu.SemaphoreType.DMA
    scratch = [
        pltpu.VMEM((1, 2048), f32),
        pltpu.VMEM((1, 512), f32),
        pltpu.VMEM((4, 1024), f32),
        pltpu.VMEM((1, 128), f32),
        pltpu.VMEM((31, 512), f32),
        pltpu.VMEM((1, 512), f32),
        pltpu.VMEM((256, 2048), bf16),
        pltpu.VMEM((8, 128, 2048), bf16),
        pltpu.VMEM((256, 2048), bf16),
        pltpu.VMEM((6, 2048, 512), bf16),
        pltpu.VMEM((4, 2, 512, 2048), bf16),
        pltpu.VMEM((6, 256, 512), bf16),
        pltpu.VMEM((2, 384, 512), bf16),
        pltpu.VMEM((2, 128, 512), f32),
        pltpu.VMEM((2, 128, 512), f32),
        pltpu.VMEM((2, 128, 512), bf16),
        pltpu.VMEM((8, 128, 512), f32),
        pltpu.VMEM((8, 128, 512), bf16),
        pltpu.VMEM((8, 128, 512), bf16),
        pltpu.VMEM((2, 128, 2048), f32),
        pltpu.VMEM((8, 128, 512), f32),
        pltpu.VMEM((8, 8, 512), f32),
        pltpu.VMEM((8, 128, 512), bf16),
        pltpu.VMEM((2, 128, 256), f32),
        pltpu.VMEM((2, 8, 256), f32),
        pltpu.VMEM((144, 256), bf16),
        pltpu.VMEM((144, 256), bf16),
        pltpu.VMEM((4, 2, 144, 128), bf16),
        pltpu.VMEM((4, 2, 144, 128), bf16),
        pltpu.VMEM((2, 2, 2, 128, 128), bf16),
        pltpu.VMEM((4, 256, 512), bf16),
        pltpu.VMEM((4, 256, 512), bf16),
        pltpu.VMEM((2, 2, 128, 512), bf16),
        pltpu.VMEM((256, 2048), f32),
        pltpu.VMEM((2, 16, 2048), bf16),
        pltpu.VMEM((1056, 512), bf16),
        pltpu.VMEM((4, 288, 512), bf16),
        pltpu.VMEM((16, 288, 128), f32),
        pltpu.VMEM((4, 256, 512), bf16),
        pltpu.VMEM((4, 32, 512), f32),
        dma((58,)),
    ]
    return pl.pallas_call(
        kernel,
        out_shape=pltpu.VMEM((256, 2048), bf16),
        in_specs=[hbm] * 15,
        out_specs=vmem,
        scratch_shapes=scratch,
        compiler_params=pltpu.CompilerParams(
            collective_id=0, has_side_effects=True, vmem_limit_bytes=60 * 1024 * 1024
        ),
    )(
        tokens,
        norm_gain[None],
        w_query,
        w_forget,
        w_value,
        w_rgate,
        w_glu_value,
        w_glu_gate,
        forget_gap[None],
        decay_shift.T,
        head_gain[None],
        conv_taps,
        conv_gain[None],
        out_rec,
        out_conv,
    )


def solution(mesh):
    placed = (
        P(("sp", "tp"), None),
        P(),
        P(None, "tp"),
        P(None, "tp"),
        P(None, "tp"),
        P(None, "tp"),
        P(None, "tp"),
        P(None, "tp"),
        P("tp"),
        P("sp", "tp"),
        P(),
        P(None, "tp"),
        P("tp"),
        P("tp", None),
        P("tp", None),
    )
    return jax.shard_map(
        on_device, mesh=mesh, in_specs=placed, out_specs=P(("sp", "tp"), None), check_vma=False
    )
```

```python
import jax
import jax.numpy as jnp
from jax import lax
from jax.experimental import pallas as pl
from jax.experimental.pallas import tpu as pltpu
from jax.sharding import PartitionSpec as P

MESH = pl.DeviceIdType.MESH
HEAD = 128
UNIT = 128
f32 = jnp.float32
bf16 = jnp.bfloat16
scope = jax.named_scope

norm_epsilon = 1e-05
head_epsilon = 1e-06

NT = (((1,), (1,)), ((), ()))
TN = (((0,), (0,)), ((), ()))


def dot(a, b):
    return jnp.dot(a, b, preferred_element_type=f32)


def split3(value):
    hi = value.astype(bf16)
    rest = value - hi.astype(f32)
    mid = rest.astype(bf16)
    low = (rest - mid.astype(f32)).astype(bf16)
    return hi, mid, low


def pack_state(state, log):
    hi, mid, low = split3(log)
    row = lax.broadcasted_iota(jnp.int32, (16, state.shape[1]), 0)
    extra = jnp.where(
        row == 0,
        hi.astype(f32),
        jnp.where(row == 1, mid.astype(f32), jnp.where(row == 2, low.astype(f32), 0.0)),
    )
    return state.astype(bf16), extra.astype(bf16)


def unpack_state(ref):
    state = ref[0:128, :].astype(f32)
    log = jnp.sum(ref[128:144, :].astype(f32), axis=0, keepdims=True)
    return state, log


def kernel(
    tokens,
    norm_gain_hbm,
    w_query,
    w_forget,
    w_value,
    w_rgate,
    w_glu_value,
    w_glu_gate,
    gap_hbm,
    shift_hbm,
    head_gain_hbm,
    taps_hbm,
    conv_gain_hbm,
    out_rec,
    out_conv,
    out,
    norm_gain,
    gap,
    shift,
    head_gain,
    taps,
    conv_gain,
    tok,
    xn,
    xp,
    w_in,
    w_rel,
    raw,
    hml,
    run,
    keys,
    kdec,
    near,
    qfar,
    rgate,
    filt,
    s_unit,
    a_unit,
    h_unit,
    s_loc,
    a_loc,
    p_send,
    p_recv,
    y_msg,
    z_msg,
    h_in,
    act,
    act_in,
    relay,
    acc,
    w_own,
    mixed_in,
    c_in,
    c_pad,
    c_act,
    tg,
    sems,
):
    x = lax.axis_index("tp")
    s = lax.axis_index("sp")
    core = lax.rem(s, 2)
    chip = s // 2
    y = lax.rem(chip, 4)
    z = chip // 4

    def around(index, step):
        return lax.rem(index + step, 4)

    right, far, left = around(x, 1), around(x, 2), around(x, 3)
    behind = lax.rem(s + 31, 32)
    ahead = lax.rem(s + 1, 32)
    partner = chip * 2 + (1 - core)

    def at_y(k):
        return (z * 4 + around(y, k)) * 2 + core

    def at_z(k):
        return (around(z, k) * 4 + y) * 2 + core

    barrier = pltpu.get_barrier_semaphore()
    peers = [{"tp": right}, {"tp": left}, {"sp": partner}, {"sp": behind}]
    peers += [{"sp": at_y(k)} for k in (1, 3)] + [{"sp": at_z(k)} for k in (1, 3)]
    for peer in peers:
        pl.semaphore_signal(barrier, inc=1, device_id=peer, device_id_type=MESH)

    def remote(src, dst, send_sem, recv_sem, target):
        return pltpu.make_async_remote_copy(
            src_ref=src,
            dst_ref=dst,
            send_sem=send_sem,
            recv_sem=recv_sem,
            device_id=target,
            device_id_type=MESH,
        )

    first_index, second_index = (y, z), (z, y)
    first_at, second_at = (at_y, at_z), (at_z, at_y)

    def slice_rows(p, j1, j2):
        return pl.ds(pl.multiple_of(16 * (core * 16 + 4 * j2 + j1), 16), 16)

    own_rows = [slice_rows(p, first_index[p], second_index[p]) for p in (0, 1)]
    weight_of = (out_rec, out_conv)

    def wait_for(ref, k):
        pltpu.make_async_copy(ref, ref, sems.at[k]).wait()

    own_loads = [
        pltpu.make_async_copy(weight_of[p].at[own_rows[p]], w_own.at[p], sems.at[9])
        for p in (0, 1)
    ]
    pairs = [(tokens, tok), (norm_gain_hbm, norm_gain)]
    pairs += [
        (weight, w_in.at[k])
        for k, weight in enumerate(
            (w_forget, w_value, w_query, w_rgate, w_glu_value, w_glu_gate)
        )
    ]
    pairs += [
        (gap_hbm, gap),
        (shift_hbm, shift),
        (head_gain_hbm, head_gain),
        (taps_hbm, taps),
        (conv_gain_hbm, conv_gain),
        (out_rec, w_rel.at[0, 0]),
        (out_conv, w_rel.at[0, 1]),
    ]
    loads = [
        pltpu.make_async_copy(src, dst, sems.at[(0, 1, 2, 2, 2, 2, 2, 2, 3, 4, 5, 6, 7, 8, 8)[k]])
        for k, (src, dst) in enumerate(pairs)
    ]
    for load in own_loads + loads:
        load.start()

    def cross(k, p, slot, src, target):
        dst = w_rel.at[slot, p, own_rows[p]]
        come = (17, 19, 19, 18, 19, 19)[k]
        return remote(src, dst, sems.at[16], sems.at[come], {"tp": target})

    def own_slice(p):
        return w_own.at[p]

    cross_out = [
        cross(0, 0, 3, own_slice(0), right),
        cross(1, 1, 3, own_slice(1), right),
        cross(2, 0, 1, own_slice(0), left),
        cross(3, 1, 1, own_slice(1), left),
        cross(4, 0, 2, w_rel.at[3, 0, own_rows[0]], right),
        cross(5, 1, 2, w_rel.at[1, 1, own_rows[1]], left),
    ]

    def packet(p, j1, j2, half):
        cols = pl.ds(0, 2048) if half is None else pl.ds(1024 * half, 1024)
        return w_rel.at[pl.ds(1, 3), p, slice_rows(p, j1, j2), cols]

    def plane(p, k, j1, j2, half, target):
        ref = packet(p, j1, j2, half)
        return remote(ref, ref, sems.at[20], sems.at[plane_sem[k]], {"sp": target})

    plane_sem = (21, 21, 22, 22, 23, 23, 26, 26, 24, 24, 26, 26, 25, 25, 26, 26, 24, 24, 26, 26)
    plane_out = []
    for p in (0, 1):
        i1, i2 = first_index[p], second_index[p]
        to1, to2 = first_at[p], second_at[p]
        sends = [
            (i1, i2, None, to1(1)),
            (i1, i2, None, to1(3)),
            (around(i1, 3), i2, 0, to1(1)),
            (around(i1, 1), i2, 1, to1(3)),
        ]
        for m in range(4):
            j1 = around(i1, m)
            sends += [
                (j1, i2, None, to2(1)),
                (j1, i2, None, to2(3)),
                (j1, around(i2, 3), 0, to2(1)),
                (j1, around(i2, 1), 1, to2(3)),
            ]
        plane_out.append([plane(p, k, *send) for k, send in enumerate(sends)])

    def twin(p, n, owner):
        j2 = around(second_index[p], (0, 3, 1, 2)[n])
        rows = pl.ds(pl.multiple_of(256 * owner + 64 * j2, 64), 64)
        ref = w_rel.at[pl.ds(1, 3), p, rows]
        return remote(ref, ref, sems.at[27], sems.at[28], {"sp": partner})

    twin_out = [[twin(p, n, core) for n in range(4)] for p in (0, 1)]

    def receive(k, rows):
        wait_for(w_rel.at[pl.ds(1, 3), 0, pl.ds(0, rows)], k)

    def start(*ks):
        for k in ks:
            for p in (1, 0):
                plane_out[p][k].start()

    def weights_0():
        wait_for(xn.at[0, pl.ds(0, 64)], 19)
        start(0, 1, 4, 5)

    def weights_1():
        receive(21, 64)
        start(2, 3)
        start(16, 17, 8, 9)

    def weights_2():
        receive(22, 32)
        start(12, 13)
        for p in (1, 0):
            twin_out[p][0].start()
        receive(23, 64)
        start(6, 7)

    def weights_3():
        receive(24, 128)
        start(18, 19, 10, 11)

    def weights_4():
        receive(25, 64)
        start(14, 15)
        for p in (1, 0):
            twin_out[p][1].start()
            twin_out[p][2].start()

    def weights_5():
        receive(26, 128)
        for p in (1, 0):
            twin_out[p][3].start()

    def norm_rows(piece):
        for row in range(0, UNIT, 32):
            wide = tok[piece * UNIT + row : piece * UNIT + row + 32, :].astype(f32)
            mean = jnp.mean(wide, axis=1, keepdims=True)
            centred = wide - mean
            var = jnp.mean(centred * centred, axis=1, keepdims=True)
            value = centred * lax.rsqrt(var + norm_epsilon) * norm_gain[...]
            xn[2 * x + piece, row : row + 32, :] = value.astype(bf16)

    def rows_copy(unit, begin, size, k, way):
        ref = xn.at[unit, pl.ds(begin, size)]
        target = {"tp": left if way else right}
        return remote(ref, ref, sems.at[10], sems.at[(11, 11, 11, 12, 13, 14, 15)[k]], target)

    parts = (
        ((1, 0, 32), (1, 32, 32), (1, 64, 64), (0, 0, 64), (0, 64, 64), (0, 0, 64), (1, 0, 64)),
        ((0, 64, 32), (0, 96, 32), (0, 0, 64), (1, 64, 64), (1, 0, 64), (0, 64, 64), (1, 64, 64)),
    )
    gather = []
    for way in (0, 1):
        source = left if way == 0 else right
        gather.append(
            [
                rows_copy(2 * (x if k < 5 else source) + u, begin, size, k, way)
                for k, (u, begin, size) in enumerate(parts[way])
            ]
        )

    def tokens_in(k):
        wait_for(xn.at[pl.ds(0, 2)] if k == 0 else xn.at[0], (11, None, None, 12, 13, 14, 15)[k])

    wait_for(w_own, 9)
    with scope("w_barrier"):
        pl.semaphore_wait(barrier, len(peers))
    for k in range(4):
        cross_out[k].start()
    with scope("w_tok"):
        loads[0].wait()
        loads[1].wait()
    with scope("ln"):
        norm_rows(0)
        norm_rows(1)
    gather[0][0].start()
    gather[1][0].start()
    with scope("w_cross"):
        cross_out[0].wait_recv()
        cross_out[4].start()
        cross_out[3].wait_recv()
        cross_out[5].start()
    for k in range(1, 5):
        gather[0][k].start()
        gather[1][k].start()

    keep = lax.broadcasted_iota(jnp.int32, (UNIT, UNIT), 0) >= lax.broadcasted_iota(
        jnp.int32, (UNIT, UNIT), 1
    )
    ones_low = jnp.where(keep, 1.0, 0.0).astype(bf16)
    tri = jnp.concatenate([ones_low, ones_low, ones_low], axis=1)

    def lanes(h):
        return slice(h * HEAD, (h + 1) * HEAD)

    def units_of(step):
        unit_a = jnp.where(step == 0, 2 * x, jnp.where(step == 1, 2 * left + 1, 2 * left))
        unit_b = jnp.where(step == 0, 2 * x + 1, jnp.where(step == 1, 2 * right, 2 * right + 1))
        return unit_a, unit_b

    def project(*ks):
        for k in ks:
            raw[k] = dot(xp[...], w_in[k]).astype(bf16)

    def each_unit(unit_a, unit_b, body):
        for k, unit in enumerate((unit_a, unit_b)):
            body(k, unit, pl.ds(k * UNIT, UNIT))

    def gates(k, unit, rows):
        for h in range(4):
            forget = raw[0, rows, lanes(h)].astype(f32)
            gate = gap[:, lanes(h)] * jax.nn.sigmoid(-forget)
            hi, mid, low = split3(jnp.log1p(-gate))
            hml[k, 0:UNIT, lanes(h)] = hi
            hml[k, UNIT : 2 * UNIT, lanes(h)] = mid
            hml[k, 2 * UNIT : 3 * UNIT, lanes(h)] = low
            keys[k, :, lanes(h)] = gate
        shifts = shift[:, pl.ds(pl.multiple_of(unit * UNIT, UNIT), UNIT)]
        shifts = jnp.concatenate(split3(shifts), axis=1)
        shift_run = lax.dot_general(tri, shifts, NT, preferred_element_type=f32)
        total = dot(tri, hml[k])
        for h in range(4):
            run_h = total[:, lanes(h)] + shift_run[:, h : h + 1]
            run[k, :, lanes(h)] = run_h
            centre = run_h[63:64, :]
            end = run_h[127:128, :]
            a_unit[unit, :, lanes(h)] = jnp.broadcast_to(end, (8, HEAD))
            decayed = keys[k, :, lanes(h)] * jnp.exp(centre - run_h)
            kdec[k, :, lanes(h)] = decayed.astype(bf16)
            ending = (decayed * jnp.exp(end - centre)).astype(bf16)
            s_unit[unit, :, lanes(h)] = lax.dot_general(
                raw[1, rows, lanes(h)], ending, TN, preferred_element_type=f32
            )

    def mix(k, unit, rows):
        value = raw[4, rows, :].astype(f32)
        mixed = value * jax.nn.sigmoid(raw[5, rows, :].astype(f32))
        mixed_in[pl.ds(pl.multiple_of(32 + unit * UNIT, 32), UNIT), :] = mixed.astype(bf16)

    def scan(k, unit, rows):
        for h in range(4):
            run_h = run[k, :, lanes(h)]
            centre = run_h[63:64, :]
            query = raw[2, rows, lanes(h)].astype(f32)
            query = query * jax.nn.sigmoid(query) * jnp.exp(run_h - centre)
            qfar[unit, :, lanes(h)] = (query * jnp.exp(centre)).astype(bf16)
            scores = lax.dot_general(
                query.astype(bf16), kdec[k, :, lanes(h)], NT, preferred_element_type=f32
            )
            scores = jnp.where(keep, scores, 0.0).astype(bf16)
            near[unit, :, lanes(h)] = dot(scores, raw[1, rows, lanes(h)])
            rgate[unit, :, lanes(h)] = raw[3, rows, lanes(h)]

    def sp_copy(ref, dst, send, come, target):
        return remote(ref, dst, sems.at[send], sems.at[come], {"sp": target})

    edge = sp_copy(mixed_in.at[pl.ds(1024, 32)], mixed_in.at[pl.ds(0, 32)], 31, 32, ahead)

    def send_edge(owner):
        @pl.when(x == owner)
        def _():
            edge.start()

    def rows_of(o, begin, size):
        return mixed_in.at[pl.ds(pl.multiple_of(256 * around(x, o) + begin, 32), size)]

    def hop(p, k, src, dst, target):
        send = (52, 44, 50)[p]
        come = 51 if p == 2 else (53, 45)[p] + (0, 1, 2, 2, 3, 3, 4, 4)[k]
        return remote(src, dst, sems.at[send], sems.at[come], {"tp": target})

    low, high = pl.ds(0, UNIT), pl.ds(UNIT, UNIT)
    low_in, high_in = pl.ds(32, UNIT), pl.ds(32 + UNIT, UNIT)
    gated = [
        hop(1, 0, rows_of(2, 32, UNIT), relay.at[1, 0], left),
        hop(1, 1, rows_of(2, 32 + UNIT, UNIT), relay.at[1, 1], right),
        hop(1, 2, rows_of(1, 32, UNIT), c_in.at[3, low_in], right),
        hop(1, 3, rows_of(1, 32 + UNIT, UNIT), c_in.at[3, high_in], right),
        hop(1, 4, rows_of(3, 32, UNIT), c_in.at[1, low_in], left),
        hop(1, 5, rows_of(3, 32 + UNIT, UNIT), c_in.at[1, high_in], left),
        hop(1, 6, relay.at[1, 0], c_in.at[2, low_in], left),
        hop(1, 7, relay.at[1, 1], c_in.at[2, high_in], right),
    ]
    edges = [
        hop(2, o, rows_of(o, 0, 32), c_in.at[4 - o, pl.ds(0, 32)], {1: right, 2: far, 3: left}[o])
        for o in (1, 2, 3)
    ]
    acts = [
        hop(0, 0, act.at[2, low], relay.at[0, 0], left),
        hop(0, 1, act.at[2, high], relay.at[0, 1], right),
        hop(0, 2, act.at[1, low], act_in.at[3, low], right),
        hop(0, 3, act.at[1, high], act_in.at[3, high], right),
        hop(0, 4, act.at[3, low], act_in.at[1, low], left),
        hop(0, 5, act.at[3, high], act_in.at[1, high], left),
        hop(0, 6, relay.at[0, 0], act_in.at[2, low], left),
        hop(0, 7, relay.at[0, 1], act_in.at[2, high], right),
    ]
    filters = [
        remote(tg.at[0], tg.at[4 - j], sems.at[42], sems.at[43], {"tp": around(x, j)})
        for j in (1, 2, 3)
    ]

    @pl.loop(0, 3)
    def _(step):
        unit_a, unit_b = units_of(step)

        @pl.when(step == 0)
        def _():
            with scope("w_weights"):
                wait_for(w_in, 2)
                for k in range(8, 13):
                    loads[k].wait()
            tg[0, 0:31, :] = taps[...]
            tg[0, 31:32, :] = conv_gain[...]

        @pl.when(step == 1)
        def _():
            with scope("w_ag1"):
                tokens_in(0)
                gather[1][5].start()

        @pl.when(step == 2)
        def _():
            with scope("w_ag2"):
                tokens_in(3)
                gather[0][5].start()
                gather[0][6].start()
                gather[1][6].start()
                tokens_in(4)
            with scope("w_w2"):
                weights_2()

        with scope("proj_fv"):
            xp[0:UNIT, :] = xn[unit_a]
            xp[UNIT : 2 * UNIT, :] = xn[unit_b]
            project(0, 1)

        @pl.when(step == 1)
        def _():
            with scope("w_w1"):
                weights_1()

        with scope("gates"):
            each_unit(unit_a, unit_b, gates)

        with scope("proj_rest"):
            project(2, 3, 4, 5)

        @pl.when(step == 0)
        def _():
            with scope("w_w0"):
                weights_0()

        with scope("scan"):
            each_unit(unit_a, unit_b, mix)
            each_unit(unit_a, unit_b, scan)

        @pl.when(step == 0)
        def _():
            send_edge(3)

        @pl.when(step == 1)
        def _():
            send_edge(0)

        @pl.when(step == 2)
        def _():
            send_edge(2)

    unit_rows = pl.ds(0, UNIT)

    def project_unit(unit, *ks):
        for k in ks:
            raw[k, 0:UNIT, :] = dot(xn[unit], w_in[k]).astype(bf16)

    with scope("w_w3_31"):
        weights_3()
    with scope("w_far_a"):
        tokens_in(5)
    with scope("far_a"):
        project_unit(2 * far, 0, 1)
        gates(0, 2 * far, unit_rows)
        project_unit(2 * far, 2, 3, 4, 5)
        mix(0, 2 * far, unit_rows)
        scan(0, 2 * far, unit_rows)
    with scope("w_far_b"):
        tokens_in(6)
    for copy in filters:
        copy.start()
    for k in (0, 2, 5, 4):
        gated[k].start()
    with scope("far_b"):
        project_unit(2 * far + 1, 0, 1)
        gates(0, 2 * far + 1, unit_rows)

    pair = sp_copy(p_send, p_recv, 29, 30, partner)
    along_y = [
        [sp_copy(y_msg.at[y, hd], y_msg.at[y, hd], 33, 34 + hd, at_y(k)) for k in (2, 1, 3)]
        for hd in (0, 1)
    ]
    along_z = [
        [sp_copy(z_msg.at[z, hd], z_msg.at[z, hd], 36, 37 + hd, at_z(k)) for k in (2, 1, 3)]
        for hd in (0, 1)
    ]
    swap = [
        sp_copy(h_in.at[1 - core, core, hd], h_in.at[1 - core, core, hd], 39, 40 + hd, partner)
        for hd in (0, 1)
    ]

    with scope("combine"):
        state = s_unit[0]
        log = a_unit[0, 0:1, :]
        for u in range(1, 8):
            a_u = a_unit[u, 0:1, :]
            state = state * jnp.exp(a_u) + s_unit[u]
            log = log + a_u
        for half in range(2):
            part_of = slice(half * 256, half * 256 + 256)
            s_loc[half] = state[:, part_of]
            a_loc[half] = jnp.broadcast_to(log[:, part_of], (8, 256))
        body, extra = pack_state(s_loc[1 - core], a_loc[1 - core, 0:1, :])
        p_send[0:128, :] = body
        p_send[128:144, :] = extra
        pair.start()
    with scope("w_pair"):
        pair.wait_recv()
    mine, mine_log = s_loc[core], a_loc[core, 0:1, :]
    other, other_log = unpack_state(p_recv)
    first = jnp.where(core == 0, mine, other)
    first_log = jnp.where(core == 0, mine_log, other_log)
    second = jnp.where(core == 0, other, mine)
    second_log = jnp.where(core == 0, other_log, mine_log)
    s_loc[core] = first
    a_loc[core] = jnp.broadcast_to(first_log, (8, 256))
    both = first * jnp.exp(second_log) + second
    both_log = first_log + second_log
    for hd in (0, 1):
        body, extra = pack_state(both[:, lanes(hd)], both_log[:, lanes(hd)])
        y_msg[y, hd, 0:128, :] = body
        y_msg[y, hd, 128:144, :] = extra
        for copy in along_y[hd]:
            copy.start()

    with scope("proj_glu"):
        project_unit(2 * far + 1, 4, 5)
        mix(0, 2 * far + 1, unit_rows)
        send_edge(1)
        gated[1].start()
        gated[3].start()

    with scope("w_w3_2"):
        weights_4()

    with scope("proj_qr"):
        project_unit(2 * far + 1, 2, 3)
        scan(0, 2 * far + 1, unit_rows)

    def widen(k, begin, size):
        if k == 0:
            source = rows_of(0, begin, size)[...]
        else:
            source = c_in[k, begin : begin + size, :]
        for g in range(4):
            c_pad[4 * k + g, begin : begin + size, :] = source[:, lanes(g)].astype(f32)

    def filter_rows(k, u):
        for g in range(4):
            total = jnp.zeros((UNIT, HEAD), f32)
            for j in range(31):
                begin = u * UNIT + 2 + j
                total = (
                    total
                    + tg[k, j : j + 1, lanes(g)] * c_pad[4 * k + g, begin : begin + UNIT, :]
                )
            filt[u, :, lanes(4 * k + g)] = total

    for hd in (0, 1):
        with scope("w_y"):
            wait_for(y_msg.at[pl.ds(0, 3), hd], 34 + hd)
        whole = jnp.zeros((128, HEAD), f32)
        whole_log = jnp.zeros((1, HEAD), f32)
        before = jnp.zeros((128, HEAD), f32)
        before_log = jnp.zeros((1, HEAD), f32)
        for k in range(4):
            state, log = unpack_state(y_msg.at[k, hd])
            before = jnp.where(k == y, whole, before)
            before_log = jnp.where(k == y, whole_log, before_log)
            whole = whole * jnp.exp(log) + state
            whole_log = whole_log + log
        body, extra = pack_state(whole, whole_log)
        z_msg[z, hd, 0:128, :] = body
        z_msg[z, hd, 128:144, :] = extra
        for copy in along_z[hd]:
            copy.start()
        s_loc[1 - core, :, lanes(hd)] = before
        a_loc[1 - core, :, lanes(hd)] = jnp.broadcast_to(before_log, (8, HEAD))

    with scope("w_relay_0"):
        gated[0].wait_recv()
        gated[6].start()
    with scope("w_edge"):
        edge.wait_recv()

        @pl.when(s == 0)
        def _():
            mixed_in[0:32, :] = jnp.zeros((32, 512), bf16)

    for copy in edges:
        copy.start()
    with scope("conv_0"):
        widen(0, 0, 288)
        filter_rows(0, 0)
        filter_rows(0, 1)

    with scope("w_filters"):
        wait_for(tg.at[pl.ds(0, 3)], 43)
    for hd in (0, 1):
        with scope("w_z"):
            wait_for(z_msg.at[pl.ds(0, 3), hd], 37 + hd)
        whole = jnp.zeros((128, HEAD), f32)
        before = jnp.zeros((128, HEAD), f32)
        for k in range(4):
            state, log = unpack_state(z_msg.at[k, hd])
            before = jnp.where(k == z, whole, before)
            whole = whole * jnp.exp(log) + state
        chip_in = before * jnp.exp(a_loc[1 - core, 0:1, lanes(hd)]) + s_loc[1 - core, :, lanes(hd)]
        h_in[0, core, hd] = chip_in.astype(bf16)
        h_in[1, core, hd] = (
            chip_in * jnp.exp(a_loc[core, 0:1, lanes(hd)]) + s_loc[core, :, lanes(hd)]
        ).astype(bf16)
        swap[hd].start()
        if hd == 0:
            with scope("w_relay_1"):
                gated[1].wait_recv()
                gated[7].start()

    with scope("w_swap"):
        swap[0].wait_recv()
        swap[1].wait_recv()

    with scope("h_units"):
        state = jnp.concatenate([h_in[core, h // 2, h % 2].astype(f32) for h in range(4)], axis=1)
        for u in range(8):
            h_unit[u] = state.astype(bf16)
            if u < 7:
                state = state * jnp.exp(a_unit[u, 0:1, :]) + s_unit[u]

    def finish_rec(o, k):
        unit = 2 * around(x, o) + k
        rows = slice(k * UNIT, k * UNIT + UNIT)
        for h in range(4):
            rec = near[unit, :, lanes(h)] + lax.dot_general(
                qfar[unit, :, lanes(h)],
                h_unit[unit, :, lanes(h)],
                NT,
                preferred_element_type=f32,
            )
            power = jnp.mean(rec * rec, axis=1, keepdims=True)
            gate = rgate[unit, :, lanes(h)].astype(f32)
            rec = rec * lax.rsqrt(power + head_epsilon) * head_gain[...]
            act[o, rows, lanes(h)] = (rec * (gate * jax.nn.sigmoid(gate))).astype(bf16)

    with scope("fin_rec"):
        finish_rec(2, 0)
        acts[0].start()
        finish_rec(2, 1)
        acts[1].start()
        finish_rec(1, 0)
        acts[2].start()
        finish_rec(3, 0)
        acts[4].start()
        finish_rec(1, 1)
        acts[3].start()
        finish_rec(3, 1)
        acts[5].start()
        finish_rec(0, 0)
        finish_rec(0, 1)

    with scope("w_w5"):
        weights_5()
    def add_product(source, k, p, begin):
        for c in range(4):
            cols = slice(c * 512, c * 512 + 512)
            product = dot(source, w_rel[k, p, :, cols])
            acc[:, cols] = product if begin else acc[:, cols] + product

    with scope("w_gated_1"):
        wait_for(c_in.at[1, pl.ds(32, 256)], 48)
    with scope("conv_1"):
        widen(1, 32, 256)
        filter_rows(1, 1)
    with scope("w_gated_3"):
        wait_for(c_in.at[3, pl.ds(32, 256)], 47)
    with scope("conv_3"):
        widen(3, 32, 256)
        filter_rows(3, 1)
    with scope("w_edges"):
        wait_for(mixed_in.at[pl.ds(0, 96)], 51)
    with scope("conv_13"):
        widen(1, 0, 32)
        filter_rows(1, 0)
        widen(3, 0, 32)
        filter_rows(3, 0)
    with scope("w_gated_2"):
        wait_for(c_in.at[2, pl.ds(32, 256)], 49)
    with scope("conv_2"):
        widen(2, 0, 288)
        filter_rows(2, 0)
        filter_rows(2, 1)
    with scope("w_relay_rec"):
        acts[0].wait_recv()
        acts[6].start()
        acts[1].wait_recv()
        acts[7].start()
    with scope("fin_conv"):
        for u in range(2):
            for row in range(0, UNIT, 32):
                rows = slice(row, row + 32)
                wide = filt[u, rows, :]
                mean = jnp.mean(wide, axis=1, keepdims=True)
                centred = wide - mean
                scale = lax.rsqrt(jnp.mean(centred * centred, axis=1, keepdims=True) + norm_epsilon)
                for k in range(4):
                    conv = filt[u, rows, k * 512 : k * 512 + 512] - mean
                    conv = conv * scale * tg[k, 31:32, :]
                    c_act[k, u * UNIT + row : u * UNIT + row + 32, :] = (
                        conv * jax.nn.sigmoid(conv)
                    ).astype(bf16)
    with scope("w_twin"):
        wait_for(w_rel.at[0], 8)
        wait_for(w_rel.at[pl.ds(1, 3), 0], 28)
    with scope("dot_conv"):
        for k in range(4):
            add_product(c_act[k], k, 1, k == 0)
        add_product(act[0], 0, 0, False)
    with scope("dot_rec"):
        wait_for(act_in.at[3], 55)
        add_product(act_in[3], 3, 0, False)
        wait_for(act_in.at[1], 56)
        add_product(act_in[1], 1, 0, False)
    with scope("w_rec2"):
        wait_for(act_in.at[2], 57)
    with scope("dot_last"):
        for c in range(4):
            cols = slice(c * 512, c * 512 + 512)
            product = dot(act_in[2], w_rel[2, 0, :, cols])
            out[:, cols] = (acc[:, cols] + product).astype(bf16)

    with scope("w_sends"):
        edge.wait_send()
        pair.wait_send()
        wait_for(xn.at[pl.ds(0, 6)], 10)
        wait_for(xn.at[0, pl.ds(0, 96)], 16)
        wait_for(w_rel.at[pl.ds(1, 3), 0, pl.ds(0, 480)], 20)
        wait_for(w_rel.at[pl.ds(1, 3), 0], 27)
        wait_for(y_msg.at[pl.ds(0, 3)], 33)
        wait_for(z_msg.at[pl.ds(0, 3)], 36)
        wait_for(h_in.at[0, 0], 39)
        wait_for(tg.at[pl.ds(0, 3)], 42)
        wait_for(act, 44)
        wait_for(mixed_in.at[pl.ds(0, 96)], 50)
        wait_for(act, 52)


def on_device(
    tokens,
    norm_gain,
    w_query,
    w_forget,
    w_value,
    w_rgate,
    w_glu_value,
    w_glu_gate,
    forget_gap,
    decay_shift,
    head_gain,
    conv_taps,
    conv_gain,
    out_rec,
    out_conv,
):
    vmem = pl.BlockSpec(memory_space=pltpu.VMEM)
    hbm = pl.BlockSpec(memory_space=pl.ANY)
    dma = pltpu.SemaphoreType.DMA
    scratch = [
        pltpu.VMEM((1, 2048), f32),
        pltpu.VMEM((1, 512), f32),
        pltpu.VMEM((4, 1024), f32),
        pltpu.VMEM((1, 128), f32),
        pltpu.VMEM((31, 512), f32),
        pltpu.VMEM((1, 512), f32),
        pltpu.VMEM((256, 2048), bf16),
        pltpu.VMEM((8, 128, 2048), bf16),
        pltpu.VMEM((256, 2048), bf16),
        pltpu.VMEM((6, 2048, 512), bf16),
        pltpu.VMEM((4, 2, 512, 2048), bf16),
        pltpu.VMEM((6, 256, 512), bf16),
        pltpu.VMEM((2, 384, 512), bf16),
        pltpu.VMEM((2, 128, 512), f32),
        pltpu.VMEM((2, 128, 512), f32),
        pltpu.VMEM((2, 128, 512), bf16),
        pltpu.VMEM((8, 128, 512), f32),
        pltpu.VMEM((8, 128, 512), bf16),
        pltpu.VMEM((8, 128, 512), bf16),
        pltpu.VMEM((2, 128, 2048), f32),
        pltpu.VMEM((8, 128, 512), f32),
        pltpu.VMEM((8, 8, 512), f32),
        pltpu.VMEM((8, 128, 512), bf16),
        pltpu.VMEM((2, 128, 256), f32),
        pltpu.VMEM((2, 8, 256), f32),
        pltpu.VMEM((144, 256), bf16),
        pltpu.VMEM((144, 256), bf16),
        pltpu.VMEM((4, 2, 144, 128), bf16),
        pltpu.VMEM((4, 2, 144, 128), bf16),
        pltpu.VMEM((2, 2, 2, 128, 128), bf16),
        pltpu.VMEM((4, 256, 512), bf16),
        pltpu.VMEM((4, 256, 512), bf16),
        pltpu.VMEM((2, 2, 128, 512), bf16),
        pltpu.VMEM((256, 2048), f32),
        pltpu.VMEM((2, 16, 2048), bf16),
        pltpu.VMEM((1056, 512), bf16),
        pltpu.VMEM((4, 288, 512), bf16),
        pltpu.VMEM((16, 288, 128), f32),
        pltpu.VMEM((4, 256, 512), bf16),
        pltpu.VMEM((4, 32, 512), f32),
        dma((58,)),
    ]
    return pl.pallas_call(
        kernel,
        out_shape=pltpu.VMEM((256, 2048), bf16),
        in_specs=[hbm] * 15,
        out_specs=vmem,
        scratch_shapes=scratch,
        compiler_params=pltpu.CompilerParams(
            collective_id=0, has_side_effects=True, vmem_limit_bytes=60 * 1024 * 1024
        ),
    )(
        tokens,
        norm_gain[None],
        w_query,
        w_forget,
        w_value,
        w_rgate,
        w_glu_value,
        w_glu_gate,
        forget_gap[None],
        decay_shift.T,
        head_gain[None],
        conv_taps,
        conv_gain[None],
        out_rec,
        out_conv,
    )


def solution(mesh):
    placed = (
        P(("sp", "tp"), None),
        P(),
        P(None, "tp"),
        P(None, "tp"),
        P(None, "tp"),
        P(None, "tp"),
        P(None, "tp"),
        P(None, "tp"),
        P("tp"),
        P("sp", "tp"),
        P(),
        P(None, "tp"),
        P("tp"),
        P("tp", None),
        P("tp", None),
    )
    return jax.shard_map(
        on_device, mesh=mesh, in_specs=placed, out_specs=P(("sp", "tp"), None), check_vma=False
    )
```
